512 devices in a mesh: ep: 32 (over z, x), tp: 16 (over y, core).
Axes of the slice: x: 4, y: 8, z: 8, core: 2. Of those that a mesh axis runs over, the one named last changes fastest.
Arguments:
- x_in: bfloat16 [4096, 12288], P('tp', 'ep'), may hold values from -6 to 6
- z_in: bfloat16 [4096, 12288], P('tp', 'ep'), may hold values from -6 to 6
- dt_raw: float32 [64, 12288], P('tp', 'ep'), may hold values from -6 to 6
- decay_rate: float32 [64], P('tp'), may hold values from 0 to 1, as said below
- b_in: bfloat16 [256, 12288], P(None, 'ep'), may hold values from -6 to 6
- c_in: bfloat16 [256, 12288], P(None, 'ep'), may hold values from -6 to 6
- conv_x: float32 [4096, 4], P('tp'), may hold values from -3 to 3
- conv_b: float32 [256, 4], replicated, may hold values from -3 to 3
- conv_c: float32 [256, 4], replicated, may hold values from -3 to 3
- head_gain: float32 [4096], P('tp'), may hold values from 0.1 to 1.9
- moe_rows: bfloat16 [5120, 2048], P('ep'), may hold values from -6 to 6
- moe_gain: float32 [2048], replicated, may hold values from 0.1 to 1.9
- routes: int32 [5120, 2], P('ep'), may hold values from 0 to 31, all different within a row; in each aligned block of 160 rows (0 to 159, 160 to 319, ...) at most 20 rows name the same one
- route_logit: float32 [5120, 2], P('ep'), may hold values from -6 to 6
- w_gate: bfloat16 [32, 2048, 5120], P('ep', None, 'tp'), may hold values from -0.125 to 0.125
- w_up: bfloat16 [32, 2048, 5120], P('ep', None, 'tp'), may hold values from -0.125 to 0.125
- w_down: bfloat16 [32, 5120, 2048], P('ep', 'tp'), may hold values from -0.078125 to 0.078125
Outputs:
- mixed: bfloat16 [4096, 12288], P('tp', 'ep')
- moe_out: bfloat16 [2048, 5120], P('tp', 'ep')
The draws below stay inside these ranges and needn't reach their ends.
Inputs may be any that keep to these rules, and one draw needn't show every extreme that they name: `routes`: each row names 2 different experts; among the rows of one index of ep no expert is named more than 20 times, a bound that some block reaches. `decay_rate`: positive rates.
All inputs are finite; a program needn't handle non-finite values.
Results may differ from the reference program's by a relative error of at most 0.018.
Values may be sent and summed in bfloat16 or wider, within the bound.
No kernel may reach another device: no remote copies, remote signals or barrier semaphores. Data moves between devices by JAX's collectives and lax.ppermute only.
A program may use at most 64 MiB of HBM per device.

```python
import math
import jax
import jax.numpy as jnp
import numpy as np
from jax import lax

D = 2048
HEADS = 64
HEAD_DIM = 64
GROUPS = 2
NSTATE = 128
KCONV = 4
BLOCK = 128
FF = 5120
TOP = 2
L_DEV = 384
MOE_DEV = 160
SEQLEN = 12288
MTOK = 5120
EXPERTS = 32
CAP = 20
N_EP = 32
N_TP = 16


def draw_decay_rate(key, part):
    order_key, slow_key, fast_key = jax.random.split(jax.random.fold_in(key, 11), 3)
    fast_count = HEADS // 2
    is_fast = jax.random.permutation(order_key, HEADS) < fast_count
    slow_rate = jnp.exp(jax.random.uniform(slow_key, (HEADS,), jnp.float32, math.log(0.05 / SEQLEN), math.log(1.0 / SEQLEN)))
    fast_rate = jnp.exp(jax.random.uniform(fast_key, (HEADS,), jnp.float32, math.log(0.012), math.log(0.04)))
    return jnp.where(is_fast, fast_rate, slow_rate)


def draw_dt_raw(key, part):
    noise_key, span_key, block_key = jax.random.split(jax.random.fold_in(key, 23), 3)
    noise = jnp.clip(0.7 * jax.random.normal(noise_key, (HEADS, SEQLEN), jnp.float32), -4.0, 4.0)
    span_shift = jax.random.uniform(span_key, (HEADS, SEQLEN // L_DEV), jnp.float32, -1.5, 1.5)
    block_shift = jax.random.uniform(block_key, (HEADS, SEQLEN // BLOCK), jnp.float32, -0.5, 0.5)
    return noise + jnp.repeat(span_shift, L_DEV, axis=1) + jnp.repeat(block_shift, BLOCK, axis=1)


def levels(stream_key, extent, pieces, smallest, largest):
    loudness, own = 1.0, jax.random.fold_in(stream_key, 6)
    for axis_at, shards_of in pieces:
        steps = jnp.exp(jax.random.uniform(jax.random.fold_in(own, axis_at), (shards_of,), jnp.float32, smallest / len(pieces), largest / len(pieces)))
        loudness = loudness * jnp.repeat(steps, extent[axis_at] // shards_of).reshape([-1 if axis == axis_at else 1 for axis in range(len(extent))])
    return loudness


def assign_block(stream_key, own, number, rows, amount, top, bound, lean):
    ranking = jax.random.permutation(stream_key, amount)
    crowded, usual = portions_of(amount, rows * top, bound, lean, True), portions_of(amount, rows * top, bound, lean, False)
    places = jnp.arange(amount)

    def named(sizes, rotation):
        used = int((sizes > 0).sum())
        fixed = max(1, used // 4)
        moved = fixed + (places - fixed + rotation * (used - fixed)) % max(1, amount - fixed)
        return jnp.zeros((amount,), jnp.int32).at[ranking[jnp.where(places < fixed, places, moved)]].set(jnp.asarray(sizes, jnp.int32))

    sizes = jnp.where(number % 4 == 0, named(crowded, number // 4), named(usual, number - number // 4 - 1))
    mixed = jax.random.permutation(jax.random.fold_in(own, 3), amount)
    giver, receiver = mixed[0:amount // 2 * 2:2], mixed[1:amount // 2 * 2:2]
    slack = jnp.minimum(sizes[giver] - 1, bound - sizes[receiver]) // 2
    slack = jnp.where((giver == ranking[0]) | (receiver == ranking[0]) | (sizes[receiver] == 0), 0, jnp.maximum(slack, 0))
    moved = jax.random.randint(jax.random.fold_in(own, 4), (amount // 2,), 0, 1 << 20) % (slack + 1)
    sizes = sizes.at[giver].add(-moved).at[receiver].add(moved)
    items = jnp.searchsorted(jnp.cumsum(sizes), jnp.arange(rows * top), side="right").astype(jnp.int32)
    grid = items.reshape(top, rows).T
    grid = grid[jax.random.permutation(jax.random.fold_in(own, 1), rows)]
    rotation = jax.random.randint(jax.random.fold_in(own, 2), (rows, 1), 0, top)
    return jnp.take_along_axis(grid, (jnp.arange(top)[None, :] + rotation) % top, axis=1)


def portions_of(amount, total, most, skew, full):
    loads = [(1 << 20) // math.isqrt(grade ** skew) + 1 for grade in range(1, amount + 1)]
    largest = most if full else min(most, max(-(-total // amount), total * loads[0] // sum(loads)))
    least = 1 if total - largest >= amount - 1 else 0
    given, spare = [largest] + [least] * (amount - 1), total - largest - least * (amount - 1)
    while spare > 0:
        free = [i for i in range(1, amount) if given[i] < largest] or [i for i in range(1, amount) if given[i] < most]
        mass, left = sum([loads[i] for i in free]), spare
        for i in free:
            addition = min(most - given[i], max(1, left * loads[i] // mass), spare)
            given[i] = given[i] + addition
            spare = spare - addition
    return np.array(given)


def gaussian(own_key, dims, width, reach, shards=(), held_as=jnp.bfloat16):
    values = width * jax.random.normal(own_key, dims, jnp.float32)
    if shards:
        values = values * levels(own_key, dims, shards, -0.22, 0.18)
    return jnp.clip(values, -reach, reach).astype(held_as)


def setup_inputs(seed: int = 0) -> dict:
    key_of = jax.random.split(jax.random.key(seed), 18)
    x_in = gaussian(key_of[0], (HEADS * HEAD_DIM, SEQLEN), 1.0, 6.0, ((0, 16), (1, 32)))
    z_in = gaussian(key_of[1], (HEADS * HEAD_DIM, SEQLEN), 1.0, 6.0, ((0, 16), (1, 32)))
    dt_raw = draw_dt_raw(jax.random.fold_in(key_of[17], 71), 0)
    decay_rate = draw_decay_rate(jax.random.fold_in(key_of[17], 71), 0)
    b_in = gaussian(key_of[4], (GROUPS * NSTATE, SEQLEN), 1.0, 6.0, ((1, 32),))
    c_in = gaussian(key_of[5], (GROUPS * NSTATE, SEQLEN), 1.0, 6.0, ((1, 32),))
    conv_x = gaussian(key_of[6], (HEADS * HEAD_DIM, KCONV), KCONV ** -0.5, 3.0, ((0, 16),), jnp.float32)
    conv_b = gaussian(key_of[7], (GROUPS * NSTATE, KCONV), KCONV ** -0.5, 3.0, (), jnp.float32)
    conv_c = gaussian(key_of[8], (GROUPS * NSTATE, KCONV), KCONV ** -0.5, 3.0, (), jnp.float32)
    head_gain = jnp.clip(1.0 + 0.18 * jax.random.normal(key_of[9], (HEADS * HEAD_DIM,), jnp.float32), 0.1, 1.9)
    moe_rows = gaussian(key_of[10], (MTOK, D), 1.0, 6.0, ((0, 32),))
    moe_gain = jnp.clip(1.0 + 0.18 * jax.random.normal(key_of[11], (D,), jnp.float32), 0.1, 1.9)
    routes_keys = jax.random.split(jax.random.fold_in(key_of[12], 1), MTOK // MOE_DEV)
    routes_turns = jax.random.permutation(jax.random.fold_in(key_of[12], 3), MTOK // MOE_DEV)
    routes = jax.vmap(lambda own, number: assign_block(jax.random.fold_in(key_of[12], 2), own, number, MOE_DEV, EXPERTS, TOP, CAP, 2))(routes_keys, routes_turns).reshape((MTOK, TOP))
    route_logit = gaussian(key_of[13], (MTOK, TOP), 1.5, 6.0, ((0, 32),), jnp.float32)
    w_gate = gaussian(key_of[14], (EXPERTS, D, FF), D ** -0.5, 0.125, ((0, 32), (2, 16)))
    w_up = gaussian(key_of[15], (EXPERTS, D, FF), D ** -0.5, 0.125, ((0, 32), (2, 16)))
    w_down = gaussian(key_of[16], (EXPERTS, FF, D), FF ** -0.5, 0.078125, ((0, 32), (1, 16)))
    return dict(x_in=x_in, z_in=z_in, dt_raw=dt_raw, decay_rate=decay_rate, b_in=b_in, c_in=c_in, conv_x=conv_x, conv_b=conv_b, conv_c=conv_c, head_gain=head_gain, moe_rows=moe_rows, moe_gain=moe_gain, routes=routes, route_logit=route_logit, w_gate=w_gate, w_up=w_up, w_down=w_down)


HIGHEST = lax.Precision.HIGHEST
ROW_EPS = 0.1
HEAD_EPS = 1.0

def causal_conv(signal, weight):
    taps = weight.shape[1]
    length = signal.shape[1]
    padded = jnp.pad(signal, ((0, 0), (taps - 1, 0)))
    running = jnp.zeros(signal.shape, jnp.float32)
    for offset in range(taps):
        running = running + weight[:, offset:offset + 1] * padded[:, offset:offset + length]
    return jax.nn.silu(running)

def block_step(state_in, x_block, b_block, c_block, log_block, step_block):
    cum_log = jnp.cumsum(log_block, axis=1)
    seg_log = cum_log[:, :, None] - cum_log[:, None, :]
    causal = jnp.tril(jnp.ones((log_block.shape[1], log_block.shape[1]), bool))
    decay_mask = jnp.exp(jnp.where(causal[None], seg_log, -jnp.inf))
    scores = jnp.einsum('hnt,hns->hts', c_block, b_block, precision=HIGHEST) * decay_mask * step_block[:, None, :]
    inner_term = jnp.einsum('hts,hps->hpt', scores, x_block, precision=HIGHEST)
    carried = jnp.einsum('hnt,hpn->hpt', c_block, state_in, precision=HIGHEST) * jnp.exp(cum_log)[:, None, :]
    tail_weight = jnp.exp(cum_log[:, -1:] - cum_log) * step_block
    fresh_state = jnp.einsum('hps,hns->hpn', x_block * tail_weight[:, None, :], b_block, precision=HIGHEST)
    new_state = jnp.exp(cum_log[:, -1])[:, None, None] * state_in + fresh_state
    return (new_state, inner_term + carried)

def mixer_half(x_in, z_in, dt_raw, decay_rate, b_in, c_in, conv_x, conv_b, conv_c, head_gain):
    x_conv = causal_conv(x_in.astype(jnp.float32), conv_x.astype(jnp.float32)).reshape(HEADS, HEAD_DIM, SEQLEN)
    b_conv = causal_conv(b_in.astype(jnp.float32), conv_b.astype(jnp.float32)).reshape(GROUPS, NSTATE, SEQLEN)
    c_conv = causal_conv(c_in.astype(jnp.float32), conv_c.astype(jnp.float32)).reshape(GROUPS, NSTATE, SEQLEN)
    step_dt = jax.nn.softplus(dt_raw.astype(jnp.float32))
    log_decay = -step_dt * decay_rate.astype(jnp.float32)[:, None]
    block_count = SEQLEN // BLOCK
    per_group = HEADS // GROUPS

    def blocks(tensor):
        return jnp.moveaxis(tensor.reshape(tensor.shape[:-1] + (block_count, BLOCK)), -2, 0)

    def advance(state_in, inputs):
        x_block, b_block, c_block, log_block, step_block = inputs
        return block_step(state_in, x_block, jnp.repeat(b_block, per_group, axis=0), jnp.repeat(c_block, per_group, axis=0), log_block, step_block)
    init_state = jnp.zeros((HEADS, HEAD_DIM, NSTATE), jnp.float32)
    _, block_out = lax.scan(advance, init_state, (blocks(x_conv), blocks(b_conv), blocks(c_conv), blocks(log_decay), blocks(step_dt)))
    y_mixed = jnp.moveaxis(block_out, 0, -2).reshape(HEADS, HEAD_DIM, SEQLEN)
    gated_out = y_mixed * jax.nn.silu(z_in.astype(jnp.float32).reshape(HEADS, HEAD_DIM, SEQLEN))
    head_scale = lax.rsqrt(lax.optimization_barrier(jnp.mean(gated_out * gated_out, axis=1, keepdims=True)) + HEAD_EPS)
    normed_out = gated_out * head_scale * head_gain.astype(jnp.float32).reshape(HEADS, HEAD_DIM, 1)
    return normed_out.reshape(HEADS * HEAD_DIM, SEQLEN).astype(jnp.bfloat16)

def experts_half(moe_rows, moe_gain, routes, route_logit, w_gate, w_up, w_down):
    rows_float = moe_rows.astype(jnp.float32)
    row_scale = lax.rsqrt(lax.optimization_barrier(jnp.mean(rows_float * rows_float, axis=1, keepdims=True)) + ROW_EPS)
    normed = (rows_float * row_scale * moe_gain.astype(jnp.float32)).astype(jnp.bfloat16)
    by_source = routes.reshape(N_EP, MOE_DEV * TOP)
    hit_table = (by_source[:, :, None] == jnp.arange(EXPERTS, dtype=jnp.int32)).astype(jnp.int32)
    slot_rank = lax.optimization_barrier(jnp.sum((jnp.cumsum(hit_table, axis=1) - hit_table) * hit_table, axis=2))
    slot_index = (jnp.arange(N_EP, dtype=jnp.int32)[:, None] * CAP + slot_rank).reshape(-1).astype(jnp.int32)
    expert_index = routes.reshape(-1).astype(jnp.int32)
    token_index = (jnp.arange(MTOK * TOP, dtype=jnp.int32) // TOP).astype(jnp.int32)
    buffer = jnp.zeros((EXPERTS, N_EP * CAP, D), jnp.bfloat16).at[expert_index, slot_index].set(normed[token_index])
    block_width = FF // N_TP

    def run_expert(inputs):
        rows_in, gate_weight, up_weight, down_weight = inputs
        gate_act = jnp.dot(rows_in, gate_weight, preferred_element_type=jnp.float32)
        up_act = jnp.dot(rows_in, up_weight, preferred_element_type=jnp.float32)
        hidden = (jax.nn.silu(gate_act) * up_act).astype(jnp.bfloat16)
        running = jnp.zeros((rows_in.shape[0], D), jnp.float32)
        for part_index in range(N_TP):
            lower = part_index * block_width
            piece_sum = jnp.dot(hidden[:, lower:lower + block_width], down_weight[lower:lower + block_width], preferred_element_type=jnp.float32)
            running = running + lax.optimization_barrier(piece_sum.astype(jnp.bfloat16)).astype(jnp.float32)
        return running.astype(jnp.bfloat16)
    results = lax.map(run_expert, (buffer, w_gate, w_up, w_down))
    picked = results[expert_index, slot_index].astype(jnp.float32).reshape(MTOK, TOP, D)
    weight = jax.nn.sigmoid(route_logit - route_logit[:, ::-1])
    combined = lax.optimization_barrier(jnp.sum(picked * weight[:, :, None], axis=1))
    return combined.T.astype(jnp.bfloat16)

def reference(x_in, z_in, dt_raw, decay_rate, b_in, c_in, conv_x, conv_b, conv_c, head_gain, moe_rows, moe_gain, routes, route_logit, w_gate, w_up, w_down):
    mixed = mixer_half(x_in, z_in, dt_raw, decay_rate, b_in, c_in, conv_x, conv_b, conv_c, head_gain)
    moe_out = experts_half(moe_rows, moe_gain, routes, route_logit, w_gate, w_up, w_down)
    return (mixed, moe_out)
```

```python
import jax
import jax.numpy as jnp
from jax import lax
from jax.experimental import pallas as pl
from jax.experimental.pallas import tpu as pltpu
from jax.sharding import Mesh
from jax.sharding import PartitionSpec as P


HEADS = 64
HEAD_DIM = 64
GROUPS = 2
NSTATE = 128
EP = ("z", "x")
TP = ("y", "c")
N_EXP = 32
CAP = 20
HEAD_ROWS = 16
TAIL_ROWS = CAP - HEAD_ROWS
LANES = 128
N_BLK = 8
CHUNK = CAP * N_BLK

TAPS = 4
ROW_EPS = 0.1
HEAD_EPS = 1.0
F32 = jnp.float32
BF16 = jnp.bfloat16
MIB = 1024 * 1024


def iota(shape, dim):
    return lax.broadcasted_iota(jnp.int32, shape, dim)


def dot(a, b):
    return jnp.dot(a, b, preferred_element_type=F32)


def call(kernel, out_shape, args, flops, smem=0, hbm=0, vmem=8, scratch=()):
    specs = [pl.BlockSpec(memory_space=pltpu.SMEM)] * smem
    specs += [pl.BlockSpec(memory_space=pltpu.HBM)] * hbm
    specs += [pl.BlockSpec(memory_space=pltpu.VMEM)] * (len(args) - smem - hbm)
    return pl.pallas_call(
        kernel,
        out_shape=out_shape,
        in_specs=specs,
        out_specs=jax.tree.map(lambda _: pl.BlockSpec(memory_space=pltpu.VMEM), out_shape),
        scratch_shapes=scratch,
        compiler_params=pltpu.CompilerParams(vmem_limit_bytes=vmem * MIB),
        cost_estimate=pl.CostEstimate(flops=flops, bytes_accessed=1 << 20, transcendentals=0),
    )(*args)


def sds(shape, dtype):
    return jax.ShapeDtypeStruct(shape, dtype)


def fetch(pairs, sems):
    copies = [
        pltpu.make_async_copy(source, target, sems.at[k]) for k, (source, target) in enumerate(pairs)
    ]
    for copy in copies:
        copy.start()
    for copy in copies:
        copy.wait()


def store_main(ref, value):
    for j in range(N_BLK):
        ref[:, HEAD_ROWS * j : HEAD_ROWS * (j + 1), :] = value[
            :, LANES * j : LANES * (j + 1)
        ].reshape(N_EXP, HEAD_ROWS, LANES)


def store_tail(ref, value):
    for g in range(2):
        low = N_BLK * HEAD_ROWS + HEAD_ROWS * g
        ref[:, low : low + HEAD_ROWS, :] = value[:, LANES * g : LANES * (g + 1)].reshape(
            N_EXP, HEAD_ROWS, LANES
        )


def load_main(ref):
    return jnp.concatenate(
        [
            ref[:, HEAD_ROWS * j : HEAD_ROWS * (j + 1), :].reshape(N_EXP * HEAD_ROWS, LANES)
            for j in range(N_BLK)
        ],
        axis=1,
    )


def load_tail(ref):
    parts = []
    for g in range(2):
        low = N_BLK * HEAD_ROWS + HEAD_ROWS * g
        parts.append(ref[:, low : low + HEAD_ROWS, :].reshape(N_EXP * HEAD_ROWS, LANES))
    return jnp.concatenate(parts, axis=1)


def prep_kernel(
    core_ref, rows_hbm, gain_hbm, routes_hbm, out_ref, rows_ref, gain_ref, routes_ref, sems
):
    fetch(((rows_hbm, rows_ref), (gain_hbm, gain_ref), (routes_hbm, routes_ref)), sems)
    tokens, features = rows_ref.shape
    half = features // 2
    low = pl.multiple_of(core_ref[0] * half, half)
    rows = rows_ref[...].astype(F32)
    scale = lax.rsqrt(jnp.mean(rows * rows, axis=1, keepdims=True) + ROW_EPS)
    own = rows_ref[:, pl.ds(low, half)].astype(F32)
    normed = (own * scale * gain_ref[:, pl.ds(low, half)]).astype(BF16)
    routes = routes_ref[...]
    expert = iota((N_EXP, tokens), 0)
    picks = [(routes[k : k + 1, :] == expert).astype(F32) for k in range(2)]
    before = (iota((tokens, tokens), 0) < iota((tokens, tokens), 1)).astype(BF16)
    ranks = dot((picks[0] + picks[1]).astype(BF16), before)
    row = iota((N_EXP * HEAD_ROWS, tokens), 0)
    main = jnp.zeros((N_EXP * HEAD_ROWS, tokens), F32)
    tails = [jnp.zeros((N_EXP * HEAD_ROWS, tokens), F32) for _ in range(TAIL_ROWS)]
    for k in range(2):
        rank = jnp.sum(ranks * picks[k], axis=0, keepdims=True).astype(jnp.int32)
        start = routes[k : k + 1, :] * HEAD_ROWS
        in_main = jnp.where(rank < HEAD_ROWS, start + rank, -1)
        in_tail = jnp.where(rank >= HEAD_ROWS, start + rank - HEAD_ROWS, -1000)
        main = main + (row == in_main).astype(F32)
        for q in range(4):
            tails[q] = tails[q] + (row == in_tail + TAIL_ROWS * q).astype(F32)
    store_main(out_ref, dot(main.astype(BF16), normed).astype(BF16))
    tail = jnp.zeros((N_EXP * HEAD_ROWS, 2 * LANES), F32)
    for q in range(4):
        pair = jnp.concatenate(
            [
                normed[:, LANES * q : LANES * (q + 1)],
                normed[:, LANES * (q + 4) : LANES * (q + 5)],
            ],
            axis=1,
        )
        tail = tail + dot(tails[q].astype(BF16), pair)
    store_tail(out_ref, tail.astype(BF16))


def tail_pick(q):
    shape = (N_EXP * TAIL_ROWS, N_EXP * HEAD_ROWS)
    r, col = (iota(shape, 0), iota(shape, 1))
    source = (r // TAIL_ROWS) * HEAD_ROWS + TAIL_ROWS * q + r % TAIL_ROWS
    return (source == col).astype(BF16)


def unpacked(ref):
    tails = load_tail(ref)
    picked = [dot(tail_pick(q), tails).astype(BF16) for q in range(4)]
    tail = jnp.concatenate(
        [p[:, LANES * g : LANES * (g + 1)] for g in range(2) for p in picked], axis=1
    )
    return jnp.concatenate([load_main(ref), tail], axis=0)


def first_half_kernel(core_ref, own_ref, gate_ref, up_ref, gate_out, up_out):
    half = gate_ref.shape[1] // 2
    low = pl.multiple_of(core_ref[0] * half, half)
    rows = unpacked(own_ref)
    gate_out[...] = over_last(rows, gate_ref[:, pl.ds(low, half)])
    up_out[...] = over_last(rows, up_ref[:, pl.ds(low, half)])


def store_blocks(ref, value):
    for j in range(N_BLK):
        ref[j] = value[:, LANES * j : LANES * (j + 1)].astype(BF16)


def down_columns(down_ref, parity):
    parts = []
    for j in range(N_BLK):
        low = pl.multiple_of((2 * j + parity) * LANES, LANES)
        parts.append(down_ref[:, pl.ds(low, LANES)])
    return jnp.concatenate(parts, axis=1)


def second_half_kernel(
    core_ref, other_ref, gate_ref, up_ref, down_ref, gate_in, up_in, hidden_out, out_ref
):
    half = gate_ref.shape[1] // 2
    other = 1 - core_ref[0]
    low = pl.multiple_of(other * half, half)
    rows = unpacked(other_ref)
    gate = gate_in[...] + over_last(rows, gate_ref[:, pl.ds(low, half)])
    up = up_in[...] + over_last(rows, up_ref[:, pl.ds(low, half)])
    hidden = (gate * jax.nn.sigmoid(gate) * up).astype(BF16)
    hidden_out[...] = hidden
    store_blocks(out_ref, dot(hidden, down_columns(down_ref, other)))


def own_down_kernel(core_ref, hidden_ref, down_ref, out_ref):
    store_blocks(out_ref, dot(hidden_ref[...], down_columns(down_ref, core_ref[0])))


def collect_kernel(parts_ref, out_ref):
    total = parts_ref[0].astype(F32)
    for j in range(1, N_BLK):
        total = total + parts_ref[j].astype(F32)
    total = total.astype(BF16)
    rows = N_EXP * HEAD_ROWS
    out_ref[:, :HEAD_ROWS, :] = total[:rows].reshape(N_EXP, HEAD_ROWS, LANES)
    shape = (N_EXP * 8, N_EXP * TAIL_ROWS)
    r, col = (iota(shape, 0), iota(shape, 1))
    spread = (r // 8 * TAIL_ROWS + r % 8 == col) & (r % 8 < TAIL_ROWS)
    tail = dot(spread.astype(BF16), total[rows:]).reshape(N_EXP, 8, LANES)
    out_ref[:, HEAD_ROWS:, :] = tail.astype(BF16)


def weights_kernel(routes_ref, logit_ref, out_ref):
    tokens = routes_ref.shape[0]
    routes = routes_ref[...]
    logit = logit_ref[...]
    expert = iota((tokens, N_EXP), 1)
    picks = [(routes[:, k : k + 1] == expert).astype(F32) for k in range(2)]
    before = (iota((tokens, tokens), 1) < iota((tokens, tokens), 0)).astype(BF16)
    ranks = dot(before, (picks[0] + picks[1]).astype(BF16))
    rows = N_EXP * HEAD_ROWS
    col = iota((tokens, rows + N_EXP * 8), 1)
    total = jnp.zeros(col.shape, F32)
    for k in range(2):
        weight = jax.nn.sigmoid(logit[:, k : k + 1] - logit[:, 1 - k : 2 - k])
        rank = jnp.sum(ranks * picks[k], axis=1, keepdims=True).astype(jnp.int32)
        route = routes[:, k : k + 1]
        place = jnp.where(
            rank < HEAD_ROWS,
            route * HEAD_ROWS + rank,
            rows + route * 8 + rank - HEAD_ROWS,
        )
        total = total + jnp.where(col == place, weight, 0.0)
    high = total.astype(BF16)
    out_ref[0] = high
    out_ref[1] = (total - high.astype(F32)).astype(BF16)


def combine_kernel(back_ref, weight_ref, out_ref):
    rows = N_EXP * HEAD_ROWS
    back = jnp.concatenate(
        [
            back_ref[:, :HEAD_ROWS, :].reshape(rows, LANES),
            back_ref[:, HEAD_ROWS:, :].reshape(N_EXP * 8, LANES),
        ],
        axis=0,
    )
    out_ref[...] = (dot(weight_ref[0], back) + dot(weight_ref[1], back)).astype(BF16)


def exchange(value, axes):
    return lax.all_to_all(value, axes, split_axis=0, concat_axis=0, tiled=True)


def from_behind(value, steps):
    count = lax.axis_size(EP)
    return lax.ppermute(value, EP, [(k, k + steps) for k in range(count - steps)])


def join(after, before):
    return call(join_kernel, sds(after.shape, BF16), (after, before), 10**8, vmem=4)


def swap_cores(value):
    return lax.ppermute(value, "c", [(0, 1), (1, 0)])


def dispatch(moe_rows, moe_gain, routes):
    core = lax.axis_index("c").astype(jnp.int32)[None]
    outbox = call(
        prep_kernel,
        sds((N_EXP, CHUNK, LANES), BF16),
        (core, moe_rows, moe_gain[None, :], routes.T),
        5 * 10**8,
        smem=1,
        hbm=3,
        scratch=(
            pltpu.VMEM(moe_rows.shape, BF16),
            pltpu.VMEM((1, moe_gain.shape[0]), F32),
            pltpu.VMEM(routes.shape[::-1], jnp.int32),
            pltpu.SemaphoreType.DMA((3,)),
        ),
    )
    return core, outbox


def run_experts(core, own, w_gate, w_up, w_down):
    rows, hidden_units = (N_EXP * CAP, w_gate.shape[2])
    gate, up, down = (w_gate[0].T, w_up[0].T, w_down[0])
    other = swap_cores(own)
    half_act = sds((rows, hidden_units), F32)
    gate_act, up_act = call(
        first_half_kernel, (half_act, half_act), (core, own, gate, up), 10**9, smem=1, vmem=20
    )
    packed = sds((N_BLK, rows, LANES), BF16)
    hidden, theirs = call(
        second_half_kernel,
        (sds((rows, hidden_units), BF16), packed),
        (core, other, gate, up, down, gate_act, up_act),
        2 * 10**9,
        smem=1,
        vmem=24,
    )
    arrived = swap_cores(theirs)
    mine = call(own_down_kernel, packed, (core, hidden, down), 6 * 10**8, smem=1, vmem=16)
    return (mine.astype(F32) + arrived.astype(F32)).astype(BF16)


def rim_kernel(group_ref, x_hbm, b_hbm, c_hbm, out_ref, x_ref, b_ref, c_ref, sems):
    low = pl.multiple_of(group_ref[0] * NSTATE, NSTATE)
    length = x_hbm.shape[1]
    last = pl.ds(length - LANES, LANES)
    fetch(
        (
            (x_hbm.at[:, last], x_ref),
            (b_hbm.at[pl.ds(low, NSTATE), last], b_ref),
            (c_hbm.at[pl.ds(low, NSTATE), last], c_ref),
        ),
        sems,
    )
    rows = jnp.concatenate([r[...].astype(F32) for r in (x_ref, b_ref, c_ref)], axis=0)
    out_ref[...] = rows.T[LANES - 8 :, :].astype(BF16)


def conv(signal, rim, taps):
    length = signal.shape[1]
    joined = jnp.concatenate([rim, signal], axis=1)
    total = taps[:, TAPS - 1 : TAPS] * signal
    for back in range(1, TAPS):
        moved = pltpu.roll(joined, back, axis=1)[:, LANES : LANES + length]
        total = total + taps[:, TAPS - 1 - back : TAPS - back] * moved
    return total * jax.nn.sigmoid(total)


def upright(taps):
    return jnp.concatenate([taps, jnp.zeros((4, taps.shape[1]), F32)], axis=0).T


def over_first(a, b):
    return lax.dot_general(a, b, (((0,), (0,)), ((), ())), preferred_element_type=F32)


def over_last(a, b):
    return lax.dot_general(a, b, (((1,), (1,)), ((), ())), preferred_element_type=F32)


def local_kernel(
    group_ref, x_hbm, b_hbm, c_hbm, rim_ref, dt_ref, rate_ref, tx_ref, tb_ref, tc_ref,
    x_out, b_out, c_out, cum_out, step_out, sent_out, x_ref, b_ref, c_ref, sems,
):
    heads, length = dt_ref.shape
    values = x_ref.shape[0]
    low = pl.multiple_of(group_ref[0] * NSTATE, NSTATE)
    own = pl.ds(low, NSTATE)
    fetch(((x_hbm, x_ref), (b_hbm.at[own], b_ref), (c_hbm.at[own], c_ref)), sems)
    rim = jnp.concatenate(
        [jnp.zeros((LANES - 8, values + 2 * NSTATE), F32), rim_ref[...].astype(F32)], axis=0
    ).T
    x = conv(x_ref[...].astype(F32), rim[:values], upright(tx_ref[...]))
    b_rim = rim[values : values + NSTATE]
    b = conv(b_ref[...].astype(F32), b_rim, upright(tb_ref[:, own])).astype(BF16)
    c_rim = rim[values + NSTATE :]
    c = conv(c_ref[...].astype(F32), c_rim, upright(tc_ref[:, own])).astype(BF16)
    raw = dt_ref[...]
    step = jnp.maximum(raw, 0.0) + jnp.log1p(jnp.exp(-jnp.abs(raw)))
    cum = -step * rate_ref[...]
    lane = iota((heads, length), 1)
    move = 1
    while move < length:
        cum = cum + jnp.where(lane >= move, pltpu.roll(cum, move, axis=1), 0.0)
        move *= 2
    x16 = x.astype(BF16)
    x_out[...] = x16
    b_out[...] = b
    c_out[...] = c
    cum_out[...] = cum
    step_out[...] = step
    end = cum[:, length - 1 : length]
    tail = jnp.exp(end - cum) * step
    sends = []
    for h in range(heads):
        rows = slice(HEAD_DIM * h, HEAD_DIM * (h + 1))
        weighted = (x[rows] * tail[h : h + 1]).astype(BF16)
        state = over_last(weighted, b)
        total = jnp.exp(end[h : h + 1])
        high = total.astype(BF16).astype(F32)
        sent_out[rows, :] = state.astype(BF16)
        sends += [high, total - high]
    sent_out[heads * HEAD_DIM :, :] = in_rows(sends).astype(BF16)


def in_rows(values):
    row = iota((16, LANES), 0)
    total = jnp.zeros((16, LANES), F32)
    for k, value in enumerate(values):
        total = jnp.where(row == k, value, total)
    return total


def inner_kernel(x_ref, b_ref, c_ref, cum_ref, step_ref, y_out):
    heads, length = cum_ref.shape
    cum = cum_ref[...]
    pad = jnp.zeros((LANES - 2 * heads, length), F32)
    columns = jnp.concatenate([cum, step_ref[...], pad], axis=0).T
    score = over_first(b_ref[...], c_ref[...])
    for h in range(heads):
        rows = slice(HEAD_DIM * h, HEAD_DIM * (h + 1))
        for t in range(length // LANES):
            here = slice(LANES * t, LANES * (t + 1))
            size = LANES * (t + 1)
            gap = cum[h : h + 1, here] - columns[:size, h : h + 1]
            inside = iota((size, LANES), 0) <= iota((size, LANES), 1) + LANES * t
            decay = jnp.exp(jnp.where(inside, gap, -1e30))
            mask = score[:size, here] * decay * columns[:size, heads + h : heads + h + 1]
            y_out[rows, here] = dot(x_ref[rows, :size], mask.astype(BF16))


def join_kernel(after_ref, before_ref, out_ref):
    size = after_ref.shape[0] - 16
    after = after_ref[...].astype(F32)
    before = before_ref[...].astype(F32)
    decays = []
    for h in range(size // HEAD_DIM):
        rows = slice(HEAD_DIM * h, HEAD_DIM * (h + 1))
        pair = slice(size + 2 * h, size + 2 * h + 1)
        rest = slice(size + 2 * h + 1, size + 2 * h + 2)
        own = after[pair] + after[rest]
        out_ref[rows, :] = (after[rows] + own * before[rows]).astype(BF16)
        total = own * (before[pair] + before[rest])
        high = total.astype(BF16).astype(F32)
        decays += [high, total - high]
    out_ref[size:, :] = in_rows(decays).astype(BF16)


def mixed_kernel(y_ref, before_ref, c_ref, cum_ref, z_ref, gain_ref, out_ref):
    heads = cum_ref.shape[0]
    reach = jnp.exp(cum_ref[...])
    carried = dot(before_ref[: heads * HEAD_DIM, :], c_ref[...])
    for h in range(heads):
        rows = slice(HEAD_DIM * h, HEAD_DIM * (h + 1))
        z = z_ref[rows, :].astype(F32)
        y = y_ref[rows, :] + carried[rows] * reach[h : h + 1]
        gated = y * (z * jax.nn.sigmoid(z))
        scale = lax.rsqrt(jnp.mean(gated * gated, axis=0, keepdims=True) + HEAD_EPS)
        out_ref[rows, :] = (gated * scale * gain_ref[rows, :]).astype(BF16)


def rims_of(group, x_in, b_in, c_in):
    rows = x_in.shape[0] + 2 * NSTATE
    own = call(
        rim_kernel,
        sds((8, rows), BF16),
        (group, x_in, b_in, c_in),
        10**8,
        smem=1,
        hbm=3,
        vmem=4,
        scratch=(
            pltpu.VMEM((x_in.shape[0], LANES), BF16),
            pltpu.VMEM((NSTATE, LANES), BF16),
            pltpu.VMEM((NSTATE, LANES), BF16),
            pltpu.SemaphoreType.DMA((3,)),
        ),
    )
    return from_behind(own, 1)


def on_device(
    x_in,
    z_in,
    dt_raw,
    decay_rate,
    b_in,
    c_in,
    conv_x,
    conv_b,
    conv_c,
    head_gain,
    moe_rows,
    moe_gain,
    routes,
    route_logit,
    w_gate,
    w_up,
    w_down,
):
    heads, length = dt_raw.shape
    values = x_in.shape[0]
    core, outbox = dispatch(moe_rows, moe_gain, routes)
    group = lax.axis_index(TP) * heads // (HEADS // GROUPS)
    group = group.astype(jnp.int32)[None]
    rims = rims_of(group, x_in, b_in, c_in)
    arrived = exchange(outbox, EP)
    x_conv, b_conv, c_conv, cum, step_dt, sent = call(
        local_kernel,
        (
            sds((values, length), BF16),
            sds((NSTATE, length), BF16),
            sds((NSTATE, length), BF16),
            sds((heads, length), F32),
            sds((heads, length), F32),
            sds((values + 16, LANES), BF16),
        ),
        (
            group, x_in, b_in, c_in, rims, dt_raw, decay_rate[:, None],
            conv_x.T, conv_b.T, conv_c.T,
        ),
        2 * 10**9,
        smem=1,
        hbm=3,
        scratch=(
            pltpu.VMEM((values, length), BF16),
            pltpu.VMEM((NSTATE, length), BF16),
            pltpu.VMEM((NSTATE, length), BF16),
            pltpu.SemaphoreType.DMA((3,)),
        ),
    )
    nearest = from_behind(sent, 1)
    second = from_behind(sent, 2)
    y_local = call(
        inner_kernel,
        sds((values, length), F32),
        (x_conv, b_conv, c_conv, cum, step_dt),
        2 * 10**9,
    )
    spans = join(nearest, second)
    for steps in (2, 4, 8, 16):
        behind = from_behind(spans, steps)
        spans = join(spans, behind)
    weights = call(
        weights_kernel,
        sds((2, moe_rows.shape[0], N_EXP * (HEAD_ROWS + 8)), BF16),
        (routes, route_logit),
        10**9,
    )
    partial = run_experts(core, arrived, w_gate, w_up, w_down)
    parts = exchange(partial, "y")
    collected = call(
        collect_kernel, sds((N_EXP, HEAD_ROWS + 8, LANES), BF16), (parts,), 10**8
    )
    back = exchange(collected, EP)
    mixed = call(
        mixed_kernel,
        sds((values, length), BF16),
        (y_local, spans, c_conv, cum, z_in, head_gain[:, None]),
        2 * 10**9,
    )
    moe_out = call(
        combine_kernel, sds((moe_rows.shape[0], LANES), BF16), (back, weights), 10**8
    ).T
    return (mixed, moe_out)


def solution(mesh):
    finer = Mesh(mesh.devices.reshape(8, 4, 8, 2), ("z", "x", "y", "c"))
    in_specs = (
        P(TP, EP),
        P(TP, EP),
        P(TP, EP),
        P(TP),
        P(None, EP),
        P(None, EP),
        P(TP, None),
        P(),
        P(),
        P(TP),
        P(EP, None),
        P(),
        P(EP, None),
        P(EP, None),
        P(EP, None, TP),
        P(EP, None, TP),
        P(EP, TP, None),
    )
    out_specs = (P(TP, EP), P(TP, EP))

    return jax.shard_map(
        on_device, mesh=finer, in_specs=in_specs, out_specs=out_specs, check_vma=False
    )
```

```python
import jax
import jax.numpy as jnp
from jax import lax
from jax.experimental import pallas as pl
from jax.experimental.pallas import tpu as pltpu
from jax.sharding import Mesh
from jax.sharding import PartitionSpec as P


HEADS = 64
HEAD_DIM = 64
GROUPS = 2
NSTATE = 128
EP = ("z", "x")
TP = ("y", "c")
N_EXP = 32
CAP = 20
HEAD_ROWS = 16
TAIL_ROWS = CAP - HEAD_ROWS
LANES = 128
N_BLK = 8
CHUNK = CAP * N_BLK

TAPS = 4
ROW_EPS = 0.1
HEAD_EPS = 1.0
F32 = jnp.float32
BF16 = jnp.bfloat16
MIB = 1024 * 1024


def iota(shape, dim):
    return lax.broadcasted_iota(jnp.int32, shape, dim)


def dot(a, b):
    return jnp.dot(a, b, preferred_element_type=F32)


def call(kernel, out_shape, args, flops, smem=0, hbm=0, vmem=8, scratch=()):
    specs = [pl.BlockSpec(memory_space=pltpu.SMEM)] * smem
    specs += [pl.BlockSpec(memory_space=pltpu.HBM)] * hbm
    specs += [pl.BlockSpec(memory_space=pltpu.VMEM)] * (len(args) - smem - hbm)
    return pl.pallas_call(
        kernel,
        out_shape=out_shape,
        in_specs=specs,
        out_specs=jax.tree.map(lambda _: pl.BlockSpec(memory_space=pltpu.VMEM), out_shape),
        scratch_shapes=scratch,
        compiler_params=pltpu.CompilerParams(vmem_limit_bytes=vmem * MIB),
        cost_estimate=pl.CostEstimate(flops=flops, bytes_accessed=1 << 20, transcendentals=0),
    )(*args)


def sds(shape, dtype):
    return jax.ShapeDtypeStruct(shape, dtype)


def fetch(pairs, sems):
    copies = [
        pltpu.make_async_copy(source, target, sems.at[k]) for k, (source, target) in enumerate(pairs)
    ]
    for copy in copies:
        copy.start()
    for copy in copies:
        copy.wait()


def store_main(ref, value):
    for j in range(N_BLK):
        ref[:, HEAD_ROWS * j : HEAD_ROWS * (j + 1), :] = value[
            :, LANES * j : LANES * (j + 1)
        ].reshape(N_EXP, HEAD_ROWS, LANES)


def store_tail(ref, value):
    for g in range(2):
        low = N_BLK * HEAD_ROWS + HEAD_ROWS * g
        ref[:, low : low + HEAD_ROWS, :] = value[:, LANES * g : LANES * (g + 1)].reshape(
            N_EXP, HEAD_ROWS, LANES
        )


def load_main(ref):
    return jnp.concatenate(
        [
            ref[:, HEAD_ROWS * j : HEAD_ROWS * (j + 1), :].reshape(N_EXP * HEAD_ROWS, LANES)
            for j in range(N_BLK)
        ],
        axis=1,
    )


def load_tail(ref):
    parts = []
    for g in range(2):
        low = N_BLK * HEAD_ROWS + HEAD_ROWS * g
        parts.append(ref[:, low : low + HEAD_ROWS, :].reshape(N_EXP * HEAD_ROWS, LANES))
    return jnp.concatenate(parts, axis=1)


def prep_kernel(
    core_ref, rows_hbm, gain_hbm, routes_hbm, out_ref, rows_ref, gain_ref, routes_ref, sems
):
    fetch(((rows_hbm, rows_ref), (gain_hbm, gain_ref), (routes_hbm, routes_ref)), sems)
    tokens, features = rows_ref.shape
    half = features // 2
    low = pl.multiple_of(core_ref[0] * half, half)
    rows = rows_ref[...].astype(F32)
    scale = lax.rsqrt(jnp.mean(rows * rows, axis=1, keepdims=True) + ROW_EPS)
    own = rows_ref[:, pl.ds(low, half)].astype(F32)
    normed = (own * scale * gain_ref[:, pl.ds(low, half)]).astype(BF16)
    routes = routes_ref[...]
    expert = iota((N_EXP, tokens), 0)
    picks = [(routes[k : k + 1, :] == expert).astype(F32) for k in range(2)]
    before = (iota((tokens, tokens), 0) < iota((tokens, tokens), 1)).astype(BF16)
    ranks = dot((picks[0] + picks[1]).astype(BF16), before)
    row = iota((N_EXP * HEAD_ROWS, tokens), 0)
    main = jnp.zeros((N_EXP * HEAD_ROWS, tokens), F32)
    tails = [jnp.zeros((N_EXP * HEAD_ROWS, tokens), F32) for _ in range(TAIL_ROWS)]
    for k in range(2):
        rank = jnp.sum(ranks * picks[k], axis=0, keepdims=True).astype(jnp.int32)
        start = routes[k : k + 1, :] * HEAD_ROWS
        in_main = jnp.where(rank < HEAD_ROWS, start + rank, -1)
        in_tail = jnp.where(rank >= HEAD_ROWS, start + rank - HEAD_ROWS, -1000)
        main = main + (row == in_main).astype(F32)
        for q in range(4):
            tails[q] = tails[q] + (row == in_tail + TAIL_ROWS * q).astype(F32)
    store_main(out_ref, dot(main.astype(BF16), normed).astype(BF16))
    tail = jnp.zeros((N_EXP * HEAD_ROWS, 2 * LANES), F32)
    for q in range(4):
        pair = jnp.concatenate(
            [
                normed[:, LANES * q : LANES * (q + 1)],
                normed[:, LANES * (q + 4) : LANES * (q + 5)],
            ],
            axis=1,
        )
        tail = tail + dot(tails[q].astype(BF16), pair)
    store_tail(out_ref, tail.astype(BF16))


def tail_pick(q):
    shape = (N_EXP * TAIL_ROWS, N_EXP * HEAD_ROWS)
    r, col = (iota(shape, 0), iota(shape, 1))
    source = (r // TAIL_ROWS) * HEAD_ROWS + TAIL_ROWS * q + r % TAIL_ROWS
    return (source == col).astype(BF16)


def unpacked(ref):
    tails = load_tail(ref)
    picked = [dot(tail_pick(q), tails).astype(BF16) for q in range(4)]
    tail = jnp.concatenate(
        [p[:, LANES * g : LANES * (g + 1)] for g in range(2) for p in picked], axis=1
    )
    return jnp.concatenate([load_main(ref), tail], axis=0)


def first_half_kernel(core_ref, own_ref, gate_ref, up_ref, gate_out, up_out):
    half = gate_ref.shape[1] // 2
    low = pl.multiple_of(core_ref[0] * half, half)
    rows = unpacked(own_ref)
    gate_out[...] = over_last(rows, gate_ref[:, pl.ds(low, half)])
    up_out[...] = over_last(rows, up_ref[:, pl.ds(low, half)])


def store_blocks(ref, value):
    for j in range(N_BLK):
        ref[j] = value[:, LANES * j : LANES * (j + 1)].astype(BF16)


def down_columns(down_ref, parity):
    parts = []
    for j in range(N_BLK):
        low = pl.multiple_of((2 * j + parity) * LANES, LANES)
        parts.append(down_ref[:, pl.ds(low, LANES)])
    return jnp.concatenate(parts, axis=1)


def second_half_kernel(
    core_ref, other_ref, gate_ref, up_ref, down_ref, gate_in, up_in, hidden_out, out_ref
):
    half = gate_ref.shape[1] // 2
    other = 1 - core_ref[0]
    low = pl.multiple_of(other * half, half)
    rows = unpacked(other_ref)
    gate = gate_in[...] + over_last(rows, gate_ref[:, pl.ds(low, half)])
    up = up_in[...] + over_last(rows, up_ref[:, pl.ds(low, half)])
    hidden = (gate * jax.nn.sigmoid(gate) * up).astype(BF16)
    hidden_out[...] = hidden
    store_blocks(out_ref, dot(hidden, down_columns(down_ref, other)))


def own_down_kernel(core_ref, hidden_ref, down_ref, out_ref):
    store_blocks(out_ref, dot(hidden_ref[...], down_columns(down_ref, core_ref[0])))


def collect_kernel(parts_ref, out_ref):
    total = parts_ref[0].astype(F32)
    for j in range(1, N_BLK):
        total = total + parts_ref[j].astype(F32)
    total = total.astype(BF16)
    rows = N_EXP * HEAD_ROWS
    out_ref[:, :HEAD_ROWS, :] = total[:rows].reshape(N_EXP, HEAD_ROWS, LANES)
    shape = (N_EXP * 8, N_EXP * TAIL_ROWS)
    r, col = (iota(shape, 0), iota(shape, 1))
    spread = (r // 8 * TAIL_ROWS + r % 8 == col) & (r % 8 < TAIL_ROWS)
    tail = dot(spread.astype(BF16), total[rows:]).reshape(N_EXP, 8, LANES)
    out_ref[:, HEAD_ROWS:, :] = tail.astype(BF16)


def weights_kernel(routes_ref, logit_ref, out_ref):
    tokens = routes_ref.shape[0]
    routes = routes_ref[...]
    logit = logit_ref[...]
    expert = iota((tokens, N_EXP), 1)
    picks = [(routes[:, k : k + 1] == expert).astype(F32) for k in range(2)]
    before = (iota((tokens, tokens), 1) < iota((tokens, tokens), 0)).astype(BF16)
    ranks = dot(before, (picks[0] + picks[1]).astype(BF16))
    rows = N_EXP * HEAD_ROWS
    col = iota((tokens, rows + N_EXP * 8), 1)
    total = jnp.zeros(col.shape, F32)
    for k in range(2):
        weight = jax.nn.sigmoid(logit[:, k : k + 1] - logit[:, 1 - k : 2 - k])
        rank = jnp.sum(ranks * picks[k], axis=1, keepdims=True).astype(jnp.int32)
        route = routes[:, k : k + 1]
        place = jnp.where(
            rank < HEAD_ROWS,
            route * HEAD_ROWS + rank,
            rows + route * 8 + rank - HEAD_ROWS,
        )
        total = total + jnp.where(col == place, weight, 0.0)
    high = total.astype(BF16)
    out_ref[0] = high
    out_ref[1] = (total - high.astype(F32)).astype(BF16)


def combine_kernel(back_ref, weight_ref, out_ref):
    rows = N_EXP * HEAD_ROWS
    back = jnp.concatenate(
        [
            back_ref[:, :HEAD_ROWS, :].reshape(rows, LANES),
            back_ref[:, HEAD_ROWS:, :].reshape(N_EXP * 8, LANES),
        ],
        axis=0,
    )
    out_ref[...] = (dot(weight_ref[0], back) + dot(weight_ref[1], back)).astype(BF16)


def exchange(value, axes):
    return lax.all_to_all(value, axes, split_axis=0, concat_axis=0, tiled=True)


def from_behind(value, steps):
    count = lax.axis_size(EP)
    return lax.ppermute(value, EP, [(k, k + steps) for k in range(count - steps)])


def join(after, before):
    return call(join_kernel, sds(after.shape, BF16), (after, before), 10**8, vmem=4)


def swap_cores(value):
    return lax.ppermute(value, "c", [(0, 1), (1, 0)])


def dispatch(moe_rows, moe_gain, routes):
    core = lax.axis_index("c").astype(jnp.int32)[None]
    outbox = call(
        prep_kernel,
        sds((N_EXP, CHUNK, LANES), BF16),
        (
            core,
            *(
                pltpu.with_memory_space_constraint(a, pltpu.HBM)
                for a in (moe_rows, moe_gain[None, :], routes.T)
            ),
        ),
        5 * 10**8,
        smem=1,
        hbm=3,
        scratch=(
            pltpu.VMEM(moe_rows.shape, BF16),
            pltpu.VMEM((1, moe_gain.shape[0]), F32),
            pltpu.VMEM(routes.shape[::-1], jnp.int32),
            pltpu.SemaphoreType.DMA((3,)),
        ),
    )
    return core, outbox


def run_experts(core, own, w_gate, w_up, w_down):
    rows, hidden_units = (N_EXP * CAP, w_gate.shape[2])
    gate, up, down = (w_gate[0].T, w_up[0].T, w_down[0])
    other = swap_cores(own)
    half_act = sds((rows, hidden_units), F32)
    gate_act, up_act = call(
        first_half_kernel, (half_act, half_act), (core, own, gate, up), 10**9, smem=1, vmem=20
    )
    packed = sds((N_BLK, rows, LANES), BF16)
    hidden, theirs = call(
        second_half_kernel,
        (sds((rows, hidden_units), BF16), packed),
        (core, other, gate, up, down, gate_act, up_act),
        2 * 10**9,
        smem=1,
        vmem=24,
    )
    arrived = swap_cores(theirs)
    mine = call(own_down_kernel, packed, (core, hidden, down), 6 * 10**8, smem=1, vmem=16)
    return (mine.astype(F32) + arrived.astype(F32)).astype(BF16)


def rim_kernel(group_ref, x_hbm, b_hbm, c_hbm, out_ref, x_ref, b_ref, c_ref, sems):
    low = pl.multiple_of(group_ref[0] * NSTATE, NSTATE)
    length = x_hbm.shape[1]
    last = pl.ds(length - LANES, LANES)
    fetch(
        (
            (x_hbm.at[:, last], x_ref),
            (b_hbm.at[pl.ds(low, NSTATE), last], b_ref),
            (c_hbm.at[pl.ds(low, NSTATE), last], c_ref),
        ),
        sems,
    )
    rows = jnp.concatenate([r[...].astype(F32) for r in (x_ref, b_ref, c_ref)], axis=0)
    out_ref[...] = rows.T[LANES - 8 :, :].astype(BF16)


def conv(signal, rim, taps):
    length = signal.shape[1]
    joined = jnp.concatenate([rim, signal], axis=1)
    total = taps[:, TAPS - 1 : TAPS] * signal
    for back in range(1, TAPS):
        moved = pltpu.roll(joined, back, axis=1)[:, LANES : LANES + length]
        total = total + taps[:, TAPS - 1 - back : TAPS - back] * moved
    return total * jax.nn.sigmoid(total)


def upright(taps):
    return jnp.concatenate([taps, jnp.zeros((4, taps.shape[1]), F32)], axis=0).T


def over_first(a, b):
    return lax.dot_general(a, b, (((0,), (0,)), ((), ())), preferred_element_type=F32)


def over_last(a, b):
    return lax.dot_general(a, b, (((1,), (1,)), ((), ())), preferred_element_type=F32)


def local_kernel(
    group_ref, x_hbm, b_hbm, c_hbm, rim_ref, dt_ref, rate_ref, tx_ref, tb_ref, tc_ref,
    x_out, b_out, c_out, cum_out, step_out, sent_out, x_ref, b_ref, c_ref, sems,
):
    heads, length = dt_ref.shape
    values = x_ref.shape[0]
    low = pl.multiple_of(group_ref[0] * NSTATE, NSTATE)
    own = pl.ds(low, NSTATE)
    fetch(((x_hbm, x_ref), (b_hbm.at[own], b_ref), (c_hbm.at[own], c_ref)), sems)
    rim = jnp.concatenate(
        [jnp.zeros((LANES - 8, values + 2 * NSTATE), F32), rim_ref[...].astype(F32)], axis=0
    ).T
    x = conv(x_ref[...].astype(F32), rim[:values], upright(tx_ref[...]))
    b_rim = rim[values : values + NSTATE]
    b = conv(b_ref[...].astype(F32), b_rim, upright(tb_ref[:, own])).astype(BF16)
    c_rim = rim[values + NSTATE :]
    c = conv(c_ref[...].astype(F32), c_rim, upright(tc_ref[:, own])).astype(BF16)
    raw = dt_ref[...]
    step = jnp.maximum(raw, 0.0) + jnp.log1p(jnp.exp(-jnp.abs(raw)))
    cum = -step * rate_ref[...]
    lane = iota((heads, length), 1)
    move = 1
    while move < length:
        cum = cum + jnp.where(lane >= move, pltpu.roll(cum, move, axis=1), 0.0)
        move *= 2
    x16 = x.astype(BF16)
    x_out[...] = x16
    b_out[...] = b
    c_out[...] = c
    cum_out[...] = cum
    step_out[...] = step
    end = cum[:, length - 1 : length]
    tail = jnp.exp(end - cum) * step
    sends = []
    for h in range(heads):
        rows = slice(HEAD_DIM * h, HEAD_DIM * (h + 1))
        weighted = (x[rows] * tail[h : h + 1]).astype(BF16)
        state = over_last(weighted, b)
        total = jnp.exp(end[h : h + 1])
        high = total.astype(BF16).astype(F32)
        sent_out[rows, :] = state.astype(BF16)
        sends += [high, total - high]
    sent_out[heads * HEAD_DIM :, :] = in_rows(sends).astype(BF16)


def in_rows(values):
    row = iota((16, LANES), 0)
    total = jnp.zeros((16, LANES), F32)
    for k, value in enumerate(values):
        total = jnp.where(row == k, value, total)
    return total


def inner_kernel(x_ref, b_ref, c_ref, cum_ref, step_ref, y_out):
    heads, length = cum_ref.shape
    cum = cum_ref[...]
    pad = jnp.zeros((LANES - 2 * heads, length), F32)
    columns = jnp.concatenate([cum, step_ref[...], pad], axis=0).T
    score = over_first(b_ref[...], c_ref[...])
    for h in range(heads):
        rows = slice(HEAD_DIM * h, HEAD_DIM * (h + 1))
        for t in range(length // LANES):
            here = slice(LANES * t, LANES * (t + 1))
            size = LANES * (t + 1)
            gap = cum[h : h + 1, here] - columns[:size, h : h + 1]
            inside = iota((size, LANES), 0) <= iota((size, LANES), 1) + LANES * t
            decay = jnp.exp(jnp.where(inside, gap, -1e30))
            mask = score[:size, here] * decay * columns[:size, heads + h : heads + h + 1]
            y_out[rows, here] = dot(x_ref[rows, :size], mask.astype(BF16))


def join_kernel(after_ref, before_ref, out_ref):
    size = after_ref.shape[0] - 16
    after = after_ref[...].astype(F32)
    before = before_ref[...].astype(F32)
    decays = []
    for h in range(size // HEAD_DIM):
        rows = slice(HEAD_DIM * h, HEAD_DIM * (h + 1))
        pair = slice(size + 2 * h, size + 2 * h + 1)
        rest = slice(size + 2 * h + 1, size + 2 * h + 2)
        own = after[pair] + after[rest]
        out_ref[rows, :] = (after[rows] + own * before[rows]).astype(BF16)
        total = own * (before[pair] + before[rest])
        high = total.astype(BF16).astype(F32)
        decays += [high, total - high]
    out_ref[size:, :] = in_rows(decays).astype(BF16)


def mixed_kernel(y_ref, before_ref, c_ref, cum_ref, z_ref, gain_ref, out_ref):
    heads = cum_ref.shape[0]
    reach = jnp.exp(cum_ref[...])
    carried = dot(before_ref[: heads * HEAD_DIM, :], c_ref[...])
    for h in range(heads):
        rows = slice(HEAD_DIM * h, HEAD_DIM * (h + 1))
        z = z_ref[rows, :].astype(F32)
        y = y_ref[rows, :] + carried[rows] * reach[h : h + 1]
        gated = y * (z * jax.nn.sigmoid(z))
        scale = lax.rsqrt(jnp.mean(gated * gated, axis=0, keepdims=True) + HEAD_EPS)
        out_ref[rows, :] = (gated * scale * gain_ref[rows, :]).astype(BF16)


def rims_of(group, x_in, b_in, c_in):
    rows = x_in.shape[0] + 2 * NSTATE
    own = call(
        rim_kernel,
        sds((8, rows), BF16),
        (group, x_in, b_in, c_in),
        10**8,
        smem=1,
        hbm=3,
        vmem=4,
        scratch=(
            pltpu.VMEM((x_in.shape[0], LANES), BF16),
            pltpu.VMEM((NSTATE, LANES), BF16),
            pltpu.VMEM((NSTATE, LANES), BF16),
            pltpu.SemaphoreType.DMA((3,)),
        ),
    )
    return from_behind(own, 1)


def on_device(
    x_in,
    z_in,
    dt_raw,
    decay_rate,
    b_in,
    c_in,
    conv_x,
    conv_b,
    conv_c,
    head_gain,
    moe_rows,
    moe_gain,
    routes,
    route_logit,
    w_gate,
    w_up,
    w_down,
):
    heads, length = dt_raw.shape
    values = x_in.shape[0]
    core, outbox = dispatch(moe_rows, moe_gain, routes)
    group = lax.axis_index(TP) * heads // (HEADS // GROUPS)
    group = group.astype(jnp.int32)[None]
    arrived = exchange(outbox, EP)
    rims = rims_of(group, x_in, b_in, c_in)
    x_conv, b_conv, c_conv, cum, step_dt, sent = call(
        local_kernel,
        (
            sds((values, length), BF16),
            sds((NSTATE, length), BF16),
            sds((NSTATE, length), BF16),
            sds((heads, length), F32),
            sds((heads, length), F32),
            sds((values + 16, LANES), BF16),
        ),
        (
            group, x_in, b_in, c_in, rims, dt_raw, decay_rate[:, None],
            conv_x.T, conv_b.T, conv_c.T,
        ),
        2 * 10**9,
        smem=1,
        hbm=3,
        scratch=(
            pltpu.VMEM((values, length), BF16),
            pltpu.VMEM((NSTATE, length), BF16),
            pltpu.VMEM((NSTATE, length), BF16),
            pltpu.SemaphoreType.DMA((3,)),
        ),
    )
    nearest = from_behind(sent, 1)
    second = from_behind(sent, 2)
    y_local = call(
        inner_kernel,
        sds((values, length), F32),
        (x_conv, b_conv, c_conv, cum, step_dt),
        2 * 10**9,
    )
    spans = join(nearest, second)
    for steps in (2, 4, 8, 16):
        behind = from_behind(spans, steps)
        spans = join(spans, behind)
    weights = call(
        weights_kernel,
        sds((2, moe_rows.shape[0], N_EXP * (HEAD_ROWS + 8)), BF16),
        (routes, route_logit),
        10**9,
    )
    partial = run_experts(core, arrived, w_gate, w_up, w_down)
    parts = exchange(partial, "y")
    collected = call(
        collect_kernel, sds((N_EXP, HEAD_ROWS + 8, LANES), BF16), (parts,), 10**8
    )
    back = exchange(collected, EP)
    mixed = call(
        mixed_kernel,
        sds((values, length), BF16),
        (y_local, spans, c_conv, cum, z_in, head_gain[:, None]),
        2 * 10**9,
    )
    moe_out = call(
        combine_kernel, sds((moe_rows.shape[0], LANES), BF16), (back, weights), 10**8
    ).T
    return (mixed, moe_out)


def solution(mesh):
    finer = Mesh(mesh.devices.reshape(8, 4, 8, 2), ("z", "x", "y", "c"))
    in_specs = (
        P(TP, EP),
        P(TP, EP),
        P(TP, EP),
        P(TP),
        P(None, EP),
        P(None, EP),
        P(TP, None),
        P(),
        P(),
        P(TP),
        P(EP, None),
        P(),
        P(EP, None),
        P(EP, None),
        P(EP, None, TP),
        P(EP, None, TP),
        P(EP, TP, None),
    )
    out_specs = (P(TP, EP), P(TP, EP))

    return jax.shard_map(
        on_device, mesh=finer, in_specs=in_specs, out_specs=out_specs, check_vma=False
    )
```

```python
import jax
import jax.numpy as jnp
from jax import lax
from jax.experimental import pallas as pl
from jax.experimental.pallas import tpu as pltpu
from jax.sharding import Mesh
from jax.sharding import PartitionSpec as P


HEADS = 64
HEAD_DIM = 64
GROUPS = 2
NSTATE = 128
EP = ("z", "x")
TP = ("y", "c")
N_EXP = 32
CAP = 20
HEAD_ROWS = 16
TAIL_ROWS = CAP - HEAD_ROWS
LANES = 128
N_BLK = 8
CHUNK = CAP * N_BLK

TAPS = 4
ROW_EPS = 0.1
HEAD_EPS = 1.0
F32 = jnp.float32
BF16 = jnp.bfloat16
MIB = 1024 * 1024


def iota(shape, dim):
    return lax.broadcasted_iota(jnp.int32, shape, dim)


def dot(a, b):
    return jnp.dot(a, b, preferred_element_type=F32)


def call(kernel, out_shape, args, flops, smem=0, hbm=0, vmem=8, scratch=()):
    specs = [pl.BlockSpec(memory_space=pltpu.SMEM)] * smem
    specs += [pl.BlockSpec(memory_space=pltpu.HBM)] * hbm
    specs += [pl.BlockSpec(memory_space=pltpu.VMEM)] * (len(args) - smem - hbm)
    return pl.pallas_call(
        kernel,
        out_shape=out_shape,
        in_specs=specs,
        out_specs=jax.tree.map(lambda _: pl.BlockSpec(memory_space=pltpu.VMEM), out_shape),
        scratch_shapes=scratch,
        compiler_params=pltpu.CompilerParams(vmem_limit_bytes=vmem * MIB),
        cost_estimate=pl.CostEstimate(flops=flops, bytes_accessed=1 << 20, transcendentals=0),
    )(*args)


def sds(shape, dtype):
    return jax.ShapeDtypeStruct(shape, dtype)


def fetch(pairs, sems):
    copies = [
        pltpu.make_async_copy(source, target, sems.at[k]) for k, (source, target) in enumerate(pairs)
    ]
    for copy in copies:
        copy.start()
    for copy in copies:
        copy.wait()


def store_main(ref, value):
    for j in range(N_BLK):
        ref[:, HEAD_ROWS * j : HEAD_ROWS * (j + 1), :] = value[
            :, LANES * j : LANES * (j + 1)
        ].reshape(N_EXP, HEAD_ROWS, LANES)


def store_tail(ref, value):
    for g in range(2):
        low = N_BLK * HEAD_ROWS + HEAD_ROWS * g
        ref[:, low : low + HEAD_ROWS, :] = value[:, LANES * g : LANES * (g + 1)].reshape(
            N_EXP, HEAD_ROWS, LANES
        )


def load_main(ref):
    return jnp.concatenate(
        [
            ref[:, HEAD_ROWS * j : HEAD_ROWS * (j + 1), :].reshape(N_EXP * HEAD_ROWS, LANES)
            for j in range(N_BLK)
        ],
        axis=1,
    )


def load_tail(ref):
    parts = []
    for g in range(2):
        low = N_BLK * HEAD_ROWS + HEAD_ROWS * g
        parts.append(ref[:, low : low + HEAD_ROWS, :].reshape(N_EXP * HEAD_ROWS, LANES))
    return jnp.concatenate(parts, axis=1)


def prep_kernel(core_ref, rows_ref, gain_ref, routes_ref, out_ref):
    tokens, features = rows_ref.shape
    half = features // 2
    low = pl.multiple_of(core_ref[0] * half, half)
    rows = rows_ref[...].astype(F32)
    scale = lax.rsqrt(jnp.mean(rows * rows, axis=1, keepdims=True) + ROW_EPS)
    own = rows_ref[:, pl.ds(low, half)].astype(F32)
    normed = (own * scale * gain_ref[:, pl.ds(low, half)]).astype(BF16)
    routes = routes_ref[...]
    expert = iota((N_EXP, tokens), 0)
    picks = [(routes[k : k + 1, :] == expert).astype(F32) for k in range(2)]
    before = (iota((tokens, tokens), 0) < iota((tokens, tokens), 1)).astype(BF16)
    ranks = dot((picks[0] + picks[1]).astype(BF16), before)
    row = iota((N_EXP * HEAD_ROWS, tokens), 0)
    main = jnp.zeros((N_EXP * HEAD_ROWS, tokens), F32)
    tails = [jnp.zeros((N_EXP * HEAD_ROWS, tokens), F32) for _ in range(TAIL_ROWS)]
    for k in range(2):
        rank = jnp.sum(ranks * picks[k], axis=0, keepdims=True).astype(jnp.int32)
        start = routes[k : k + 1, :] * HEAD_ROWS
        in_main = jnp.where(rank < HEAD_ROWS, start + rank, -1)
        in_tail = jnp.where(rank >= HEAD_ROWS, start + rank - HEAD_ROWS, -1000)
        main = main + (row == in_main).astype(F32)
        for q in range(4):
            tails[q] = tails[q] + (row == in_tail + TAIL_ROWS * q).astype(F32)
    store_main(out_ref, dot(main.astype(BF16), normed).astype(BF16))
    tail = jnp.zeros((N_EXP * HEAD_ROWS, 2 * LANES), F32)
    for q in range(4):
        pair = jnp.concatenate(
            [
                normed[:, LANES * q : LANES * (q + 1)],
                normed[:, LANES * (q + 4) : LANES * (q + 5)],
            ],
            axis=1,
        )
        tail = tail + dot(tails[q].astype(BF16), pair)
    store_tail(out_ref, tail.astype(BF16))


def tail_pick(q):
    shape = (N_EXP * TAIL_ROWS, N_EXP * HEAD_ROWS)
    r, col = (iota(shape, 0), iota(shape, 1))
    source = (r // TAIL_ROWS) * HEAD_ROWS + TAIL_ROWS * q + r % TAIL_ROWS
    return (source == col).astype(BF16)


def unpacked(ref):
    tails = load_tail(ref)
    picked = [dot(tail_pick(q), tails).astype(BF16) for q in range(4)]
    tail = jnp.concatenate(
        [p[:, LANES * g : LANES * (g + 1)] for g in range(2) for p in picked], axis=1
    )
    return jnp.concatenate([load_main(ref), tail], axis=0)


def first_half_kernel(core_ref, own_ref, gate_ref, up_ref, gate_out, up_out):
    half = gate_ref.shape[1] // 2
    low = pl.multiple_of(core_ref[0] * half, half)
    rows = unpacked(own_ref)
    gate_out[...] = over_last(rows, gate_ref[:, pl.ds(low, half)])
    up_out[...] = over_last(rows, up_ref[:, pl.ds(low, half)])


def down_columns(down_ref, parity):
    parts = []
    for j in range(N_BLK):
        low = pl.multiple_of((2 * j + parity) * LANES, LANES)
        parts.append(down_ref[:, pl.ds(low, LANES)])
    return jnp.concatenate(parts, axis=1)


def second_half_kernel(
    core_ref, other_ref, gate_ref, up_ref, gate_in, up_in, hidden_out
):
    half = gate_ref.shape[1] // 2
    other = 1 - core_ref[0]
    low = pl.multiple_of(other * half, half)
    rows = unpacked(other_ref)
    gate = gate_in[...] + over_last(rows, gate_ref[:, pl.ds(low, half)])
    up = up_in[...] + over_last(rows, up_ref[:, pl.ds(low, half)])
    hidden = (gate * jax.nn.sigmoid(gate) * up).astype(BF16)
    hidden_out[...] = hidden


def pick_kernel(core_ref, down_ref, own_out, other_out):
    own_out[...] = down_columns(down_ref, core_ref[0])
    other_out[...] = down_columns(down_ref, 1 - core_ref[0])


def own_down_kernel(hidden_ref, down_ref, out_ref):
    out_ref[...] = dot(hidden_ref[...], down_ref[...])


def other_down_kernel(hidden_ref, down_ref, own_ref, out_ref):
    value = own_ref[...] + dot(hidden_ref[...], down_ref[...])
    for j in range(N_BLK):
        out_ref[j] = value[:, LANES * j : LANES * (j + 1)].astype(BF16)


def collect_kernel(parts_ref, out_ref):
    total = parts_ref[0].astype(F32)
    for j in range(1, N_BLK):
        total = total + parts_ref[j].astype(F32)
    total = total.astype(BF16)
    rows = N_EXP * HEAD_ROWS
    out_ref[:, :HEAD_ROWS, :] = total[:rows].reshape(N_EXP, HEAD_ROWS, LANES)
    shape = (N_EXP * 8, N_EXP * TAIL_ROWS)
    r, col = (iota(shape, 0), iota(shape, 1))
    spread = (r // 8 * TAIL_ROWS + r % 8 == col) & (r % 8 < TAIL_ROWS)
    tail = dot(spread.astype(BF16), total[rows:]).reshape(N_EXP, 8, LANES)
    out_ref[:, HEAD_ROWS:, :] = tail.astype(BF16)


def weights_kernel(routes_ref, logit_ref, out_ref):
    tokens = routes_ref.shape[0]
    routes = routes_ref[...]
    logit = logit_ref[...]
    expert = iota((tokens, N_EXP), 1)
    picks = [(routes[:, k : k + 1] == expert).astype(F32) for k in range(2)]
    before = (iota((tokens, tokens), 1) < iota((tokens, tokens), 0)).astype(BF16)
    ranks = dot(before, (picks[0] + picks[1]).astype(BF16))
    rows = N_EXP * HEAD_ROWS
    col = iota((tokens, rows + N_EXP * 8), 1)
    total = jnp.zeros(col.shape, F32)
    for k in range(2):
        weight = jax.nn.sigmoid(logit[:, k : k + 1] - logit[:, 1 - k : 2 - k])
        rank = jnp.sum(ranks * picks[k], axis=1, keepdims=True).astype(jnp.int32)
        route = routes[:, k : k + 1]
        place = jnp.where(
            rank < HEAD_ROWS,
            route * HEAD_ROWS + rank,
            rows + route * 8 + rank - HEAD_ROWS,
        )
        total = total + jnp.where(col == place, weight, 0.0)
    high = total.astype(BF16)
    out_ref[0] = high
    out_ref[1] = (total - high.astype(F32)).astype(BF16)


def combine_kernel(back_ref, weight_ref, out_ref):
    rows = N_EXP * HEAD_ROWS
    back = jnp.concatenate(
        [
            back_ref[:, :HEAD_ROWS, :].reshape(rows, LANES),
            back_ref[:, HEAD_ROWS:, :].reshape(N_EXP * 8, LANES),
        ],
        axis=0,
    )
    out_ref[...] = (dot(weight_ref[0], back) + dot(weight_ref[1], back)).astype(BF16)


def exchange(value, axes):
    return lax.all_to_all(value, axes, split_axis=0, concat_axis=0, tiled=True)


def from_behind(value, steps):
    count = lax.axis_size(EP)
    return lax.ppermute(value, EP, [(k, k + steps) for k in range(count - steps)])


def rows_behind(value, steps):
    count = lax.axis_size("z")
    return lax.ppermute(value, "z", [(k, k + steps) for k in range(count - steps)])


def join(after, before):
    return call(join_kernel, sds(after.shape, BF16), (after, before), 10**8, vmem=4)


def swap_cores(value):
    return lax.ppermute(value, "c", [(0, 1), (1, 0)])


def in_hbm(*arrays):
    return tuple(pltpu.with_memory_space_constraint(a, pltpu.HBM) for a in arrays)


def first_loads(group, x_in, b_in, c_in, moe_rows, moe_gain, routes):
    rows = x_in.shape[0] + 2 * NSTATE
    given = in_hbm(x_in, b_in, c_in, moe_rows, moe_gain[None, :], routes.T)
    return call(
        rim_kernel,
        (sds((8, rows), BF16), *(sds(a.shape, a.dtype) for a in given[3:])),
        (group, *given),
        10**8,
        smem=1,
        hbm=6,
        vmem=4,
        scratch=(
            pltpu.VMEM((x_in.shape[0], LANES), BF16),
            pltpu.VMEM((NSTATE, LANES), BF16),
            pltpu.VMEM((NSTATE, LANES), BF16),
            pltpu.SemaphoreType.DMA((6,)),
        ),
    )


def down_halves(core, down):
    half = sds((down.shape[0], down.shape[1] // 2), BF16)
    own, theirs = call(pick_kernel, (half, half), (core, down), 10**8, smem=1)
    return own, swap_cores(theirs)


def run_experts(core, own, w_gate, w_up, down_own, down_other):
    rows, hidden_units = (N_EXP * CAP, w_gate.shape[2])
    gate, up = (w_gate[0].T, w_up[0].T)
    other = swap_cores(own)
    half_act = sds((rows, hidden_units), F32)
    gate_act, up_act = call(
        first_half_kernel, (half_act, half_act), (core, own, gate, up), 10**9, smem=1, vmem=20
    )
    hidden = call(
        second_half_kernel,
        sds((rows, hidden_units), BF16),
        (core, other, gate, up, gate_act, up_act),
        2 * 10**9,
        smem=1,
        vmem=20,
    )
    partner = swap_cores(hidden)
    mine = call(
        own_down_kernel,
        sds((rows, down_own.shape[1]), F32),
        (hidden, down_own),
        6 * 10**8,
        vmem=12,
    )
    return call(
        other_down_kernel,
        sds((N_BLK, rows, LANES), BF16),
        (partner, down_other, mine),
        6 * 10**8,
        vmem=12,
    )


def rim_kernel(
    group_ref, x_hbm, b_hbm, c_hbm, rows_hbm, gain_hbm, routes_hbm,
    out_ref, rows_out, gain_out, routes_out, x_ref, b_ref, c_ref, sems,
):
    group = pl.ds(pl.multiple_of(group_ref[0] * NSTATE, NSTATE), NSTATE)
    last = pl.ds(x_hbm.shape[1] - LANES, LANES)
    pairs = (
        (x_hbm.at[:, last], x_ref),
        (b_hbm.at[group, last], b_ref),
        (c_hbm.at[group, last], c_ref),
        (rows_hbm, rows_out),
        (gain_hbm, gain_out),
        (routes_hbm, routes_out),
    )
    copies = [
        pltpu.make_async_copy(source, target, sems.at[k]) for k, (source, target) in enumerate(pairs)
    ]
    for copy in copies:
        copy.start()
    for copy in copies[:3]:
        copy.wait()
    rows = jnp.concatenate([r[...].astype(F32) for r in (x_ref, b_ref, c_ref)], axis=0)
    out_ref[...] = rows.T[LANES - 8 :, :].astype(BF16)
    for copy in copies[3:]:
        copy.wait()


def conv(signal, rim, taps):
    length = signal.shape[1]
    joined = jnp.concatenate([rim, signal], axis=1)
    total = taps[:, TAPS - 1 : TAPS] * signal
    for back in range(1, TAPS):
        moved = pltpu.roll(joined, back, axis=1)[:, LANES : LANES + length]
        total = total + taps[:, TAPS - 1 - back : TAPS - back] * moved
    return total * jax.nn.sigmoid(total)


def upright(taps):
    return jnp.concatenate([taps, jnp.zeros((4, taps.shape[1]), F32)], axis=0).T


def over_first(a, b):
    return lax.dot_general(a, b, (((0,), (0,)), ((), ())), preferred_element_type=F32)


def over_last(a, b):
    return lax.dot_general(a, b, (((1,), (1,)), ((), ())), preferred_element_type=F32)


def local_kernel(
    group_ref, x_hbm, b_hbm, c_hbm, rim_ref, dt_ref, rate_ref, tx_ref, tb_ref, tc_ref,
    x_out, b_out, c_out, cum_out, step_out, sent_out, x_ref, b_ref, c_ref, sems,
):
    heads, length = dt_ref.shape
    values = x_ref.shape[0]
    low = pl.multiple_of(group_ref[0] * NSTATE, NSTATE)
    own = pl.ds(low, NSTATE)
    fetch(((x_hbm, x_ref), (b_hbm.at[own], b_ref), (c_hbm.at[own], c_ref)), sems)
    rim = jnp.concatenate(
        [jnp.zeros((LANES - 8, values + 2 * NSTATE), F32), rim_ref[...].astype(F32)], axis=0
    ).T
    x = conv(x_ref[...].astype(F32), rim[:values], upright(tx_ref[...]))
    b_rim = rim[values : values + NSTATE]
    b = conv(b_ref[...].astype(F32), b_rim, upright(tb_ref[:, own])).astype(BF16)
    c_rim = rim[values + NSTATE :]
    c = conv(c_ref[...].astype(F32), c_rim, upright(tc_ref[:, own])).astype(BF16)
    raw = dt_ref[...]
    step = jnp.maximum(raw, 0.0) + jnp.log1p(jnp.exp(-jnp.abs(raw)))
    cum = -step * rate_ref[...]
    lane = iota((heads, length), 1)
    move = 1
    while move < length:
        cum = cum + jnp.where(lane >= move, pltpu.roll(cum, move, axis=1), 0.0)
        move *= 2
    x16 = x.astype(BF16)
    x_out[...] = x16
    b_out[...] = b
    c_out[...] = c
    cum_out[...] = cum
    step_out[...] = step
    end = cum[:, length - 1 : length]
    tail = jnp.exp(end - cum) * step
    sends = []
    for h in range(heads):
        rows = slice(HEAD_DIM * h, HEAD_DIM * (h + 1))
        weighted = (x[rows] * tail[h : h + 1]).astype(BF16)
        state = over_last(weighted, b)
        total = jnp.exp(end[h : h + 1])
        high = total.astype(BF16).astype(F32)
        sent_out[rows, :] = state.astype(BF16)
        sends += [high, total - high]
    sent_out[heads * HEAD_DIM :, :] = in_rows(sends).astype(BF16)


def in_rows(values):
    row = iota((16, LANES), 0)
    total = jnp.zeros((16, LANES), F32)
    for k, value in enumerate(values):
        total = jnp.where(row == k, value, total)
    return total


def inner_kernel(x_ref, b_ref, c_ref, cum_ref, step_ref, y_out):
    heads, length = cum_ref.shape
    cum = cum_ref[...]
    pad = jnp.zeros((LANES - 2 * heads, length), F32)
    columns = jnp.concatenate([cum, step_ref[...], pad], axis=0).T
    score = over_first(b_ref[...], c_ref[...])
    for h in range(heads):
        rows = slice(HEAD_DIM * h, HEAD_DIM * (h + 1))
        for t in range(length // LANES):
            here = slice(LANES * t, LANES * (t + 1))
            size = LANES * (t + 1)
            gap = cum[h : h + 1, here] - columns[:size, h : h + 1]
            inside = iota((size, LANES), 0) <= iota((size, LANES), 1) + LANES * t
            decay = jnp.exp(jnp.where(inside, gap, -1e30))
            mask = score[:size, here] * decay * columns[:size, heads + h : heads + h + 1]
            y_out[rows, here] = dot(x_ref[rows, :size], mask.astype(BF16))


def state_and_decays(ref):
    size = ref.shape[0] - 16
    value = ref[...].astype(F32)
    pairs = range(size, size + 2 * (size // HEAD_DIM), 2)
    return value[:size], [value[k : k + 1] + value[k + 1 : k + 2] for k in pairs]


def joined(after, before):
    states = [
        after[0][HEAD_DIM * h : HEAD_DIM * (h + 1)] + d * before[0][HEAD_DIM * h : HEAD_DIM * (h + 1)]
        for h, d in enumerate(after[1])
    ]
    return jnp.concatenate(states, axis=0), [a * b for a, b in zip(after[1], before[1])]


def store_spans(ref, value):
    size = ref.shape[0] - 16
    ref[:size, :] = value[0].astype(BF16)
    rows = []
    for total in value[1]:
        high = total.astype(BF16).astype(F32)
        rows += [high, total - high]
    ref[size:, :] = in_rows(rows).astype(BF16)


def join_kernel(after_ref, before_ref, out_ref):
    store_spans(out_ref, joined(state_and_decays(after_ref), state_and_decays(before_ref)))


def row_kernel(place_ref, own_ref, first_ref, second_ref, third_ref, before_out, total_out):
    place = place_ref[0]
    sources = [state_and_decays(r) for r in (own_ref, first_ref, second_ref, third_ref)]
    heads = len(sources[0][1])
    running = (jnp.zeros(sources[0][0].shape, F32), [jnp.ones((1, LANES), F32)] * heads)
    before = running
    for j in range(4):
        back = (place - j) & 3
        state, decays = sources[0]
        for k in range(1, 4):
            here = back == k
            state = jnp.where(here, sources[k][0], state)
            decays = [jnp.where(here, a, b) for a, b in zip(sources[k][1], decays)]
        running = joined((state, decays), running)
        ahead = j < place
        before = (
            jnp.where(ahead, running[0], before[0]),
            [jnp.where(ahead, a, b) for a, b in zip(running[1], before[1])],
        )
    store_spans(before_out, before)
    store_spans(total_out, running)


def mixed_kernel(y_ref, row_ref, far_ref, c_ref, cum_ref, z_ref, gain_ref, out_ref):
    heads = cum_ref.shape[0]
    reach = jnp.exp(cum_ref[...])
    before = joined(state_and_decays(row_ref), state_and_decays(far_ref))[0]
    carried = dot(before.astype(BF16), c_ref[...])
    for h in range(heads):
        rows = slice(HEAD_DIM * h, HEAD_DIM * (h + 1))
        z = z_ref[rows, :].astype(F32)
        y = y_ref[rows, :] + carried[rows] * reach[h : h + 1]
        gated = y * (z * jax.nn.sigmoid(z))
        scale = lax.rsqrt(jnp.mean(gated * gated, axis=0, keepdims=True) + HEAD_EPS)
        out_ref[rows, :] = (gated * scale * gain_ref[rows, :]).astype(BF16)


def on_device(
    x_in,
    z_in,
    dt_raw,
    decay_rate,
    b_in,
    c_in,
    conv_x,
    conv_b,
    conv_c,
    head_gain,
    moe_rows,
    moe_gain,
    routes,
    route_logit,
    w_gate,
    w_up,
    w_down,
):
    heads, length = dt_raw.shape
    values = x_in.shape[0]
    core = lax.axis_index("c").astype(jnp.int32)[None]
    group = lax.axis_index(TP) * heads // (HEADS // GROUPS)
    group = group.astype(jnp.int32)[None]
    own_rim, *tokens = first_loads(group, x_in, b_in, c_in, moe_rows, moe_gain, routes)
    rims = from_behind(own_rim, 1)
    outbox = call(prep_kernel, sds((N_EXP, CHUNK, LANES), BF16), (core, *tokens), 5 * 10**8, smem=1)
    arrived = exchange(outbox, EP)
    down_parts = down_halves(core, w_down[0])
    x_conv, b_conv, c_conv, cum, step_dt, sent = call(
        local_kernel,
        (
            sds((values, length), BF16),
            sds((NSTATE, length), BF16),
            sds((NSTATE, length), BF16),
            sds((heads, length), F32),
            sds((heads, length), F32),
            sds((values + 16, LANES), BF16),
        ),
        (
            group, x_in, b_in, c_in, rims, dt_raw, decay_rate[:, None],
            conv_x.T, conv_b.T, conv_c.T,
        ),
        2 * 10**9,
        smem=1,
        hbm=3,
        scratch=(
            pltpu.VMEM((values, length), BF16),
            pltpu.VMEM((NSTATE, length), BF16),
            pltpu.VMEM((NSTATE, length), BF16),
            pltpu.SemaphoreType.DMA((3,)),
        ),
    )
    in_order = [
        lax.ppermute(sent, "x", [(k, (k + step) % 4) for k in range(4)]) for step in (1, 2, 3)
    ]
    y_local = call(
        inner_kernel,
        sds((values, length), F32),
        (x_conv, b_conv, c_conv, cum, step_dt),
        2 * 10**8,
    )
    in_row, spans = call(
        row_kernel,
        (sds(sent.shape, BF16), sds(sent.shape, BF16)),
        (lax.axis_index("x").astype(jnp.int32)[None], sent, *in_order),
        10**8,
        smem=1,
    )
    nearest = rows_behind(spans, 1)
    second = rows_behind(spans, 2)
    spans = join(nearest, second)
    for steps in (2, 4):
        behind = rows_behind(spans, steps)
        spans = join(spans, behind)
    weights = call(
        weights_kernel,
        sds((2, moe_rows.shape[0], N_EXP * (HEAD_ROWS + 8)), BF16),
        (routes, route_logit),
        10**9,
    )
    partial = run_experts(core, arrived, w_gate, w_up, *down_parts)
    parts = exchange(partial, "y")
    collected = call(
        collect_kernel, sds((N_EXP, HEAD_ROWS + 8, LANES), BF16), (parts,), 10**8
    )
    back = exchange(collected, EP)
    mixed = call(
        mixed_kernel,
        sds((values, length), BF16),
        (y_local, in_row, spans, c_conv, cum, z_in, head_gain[:, None]),
        2 * 10**9,
    )
    moe_out = call(
        combine_kernel, sds((moe_rows.shape[0], LANES), BF16), (back, weights), 10**8
    ).T
    return (mixed, moe_out)


def solution(mesh):
    finer = Mesh(mesh.devices.reshape(8, 4, 8, 2), ("z", "x", "y", "c"))
    in_specs = (
        P(TP, EP),
        P(TP, EP),
        P(TP, EP),
        P(TP),
        P(None, EP),
        P(None, EP),
        P(TP, None),
        P(),
        P(),
        P(TP),
        P(EP, None),
        P(),
        P(EP, None),
        P(EP, None),
        P(EP, None, TP),
        P(EP, None, TP),
        P(EP, TP, None),
    )
    out_specs = (P(TP, EP), P(TP, EP))

    return jax.shard_map(
        on_device, mesh=finer, in_specs=in_specs, out_specs=out_specs, check_vma=False
    )
```

```python
import jax
import jax.numpy as jnp
from jax import lax
from jax.experimental import pallas as pl
from jax.experimental.pallas import tpu as pltpu
from jax.sharding import Mesh
from jax.sharding import PartitionSpec as P


HEADS = 64
HEAD_DIM = 64
GROUPS = 2
NSTATE = 128
EP = ("z", "x")
TP = ("y", "c")
N_EXP = 32
CAP = 20
HEAD_ROWS = 16
TAIL_ROWS = CAP - HEAD_ROWS
LANES = 128
N_BLK = 8
CHUNK = CAP * N_BLK

TAPS = 4
ROW_EPS = 0.1
HEAD_EPS = 1.0
F32 = jnp.float32
BF16 = jnp.bfloat16
MIB = 1024 * 1024


def iota(shape, dim):
    return lax.broadcasted_iota(jnp.int32, shape, dim)


def dot(a, b):
    return jnp.dot(a, b, preferred_element_type=F32)


def call(kernel, out_shape, args, flops, smem=0, hbm=0, out_hbm=False, vmem=8, scratch=()):
    specs = [pl.BlockSpec(memory_space=pltpu.SMEM)] * smem
    specs += [pl.BlockSpec(memory_space=pltpu.HBM)] * hbm
    specs += [pl.BlockSpec(memory_space=pltpu.VMEM)] * (len(args) - smem - hbm)
    out_space = pltpu.HBM if out_hbm else pltpu.VMEM
    return pl.pallas_call(
        kernel,
        out_shape=out_shape,
        in_specs=specs,
        out_specs=jax.tree.map(lambda _: pl.BlockSpec(memory_space=out_space), out_shape),
        scratch_shapes=scratch,
        compiler_params=pltpu.CompilerParams(vmem_limit_bytes=vmem * MIB),
        cost_estimate=pl.CostEstimate(flops=flops, bytes_accessed=1 << 20, transcendentals=0),
    )(*args)


def sds(shape, dtype):
    return jax.ShapeDtypeStruct(shape, dtype)


def fetch(pairs, sems):
    copies = [
        pltpu.make_async_copy(source, target, sems.at[k]) for k, (source, target) in enumerate(pairs)
    ]
    for copy in copies:
        copy.start()
    for copy in copies:
        copy.wait()


def store_tail(ref, value):
    for g in range(2):
        low = N_BLK * HEAD_ROWS + HEAD_ROWS * g
        ref[:, low : low + HEAD_ROWS, :] = value[:, LANES * g : LANES * (g + 1)].reshape(
            N_EXP, HEAD_ROWS, LANES
        )


def load_main(ref):
    return jnp.concatenate(
        [
            ref[:, HEAD_ROWS * j : HEAD_ROWS * (j + 1), :].reshape(N_EXP * HEAD_ROWS, LANES)
            for j in range(N_BLK)
        ],
        axis=1,
    )


def load_tail(ref):
    parts = []
    for g in range(2):
        low = N_BLK * HEAD_ROWS + HEAD_ROWS * g
        parts.append(ref[:, low : low + HEAD_ROWS, :].reshape(N_EXP * HEAD_ROWS, LANES))
    return jnp.concatenate(parts, axis=1)


def prep_kernel(core_ref, rows_ref, gain_ref, routes_ref, out_hbm, out_ref, sems):
    tokens, features = rows_ref.shape
    half = features // 2
    low = pl.multiple_of(core_ref[0] * half, half)
    rows = rows_ref[...].astype(F32)
    scale = lax.rsqrt(jnp.mean(rows * rows, axis=1, keepdims=True) + ROW_EPS)
    own = rows_ref[:, pl.ds(low, half)].astype(F32)
    normed = (own * scale * gain_ref[:, pl.ds(low, half)]).astype(BF16)
    routes = routes_ref[...]
    expert = iota((N_EXP, tokens), 0)
    picks = [(routes[k : k + 1, :] == expert).astype(F32) for k in range(2)]
    before = (iota((tokens, tokens), 0) < iota((tokens, tokens), 1)).astype(BF16)
    ranks = dot((picks[0] + picks[1]).astype(BF16), before)
    row = iota((N_EXP * HEAD_ROWS, tokens), 0)
    places = []
    for k in range(2):
        rank = jnp.sum(ranks * picks[k], axis=0, keepdims=True).astype(jnp.int32)
        start = routes[k : k + 1, :] * HEAD_ROWS
        places.append(
            (
                jnp.where(rank < HEAD_ROWS, start + rank, -1),
                jnp.where(rank >= HEAD_ROWS, start + rank - HEAD_ROWS, -1000),
            )
        )

    def one_hot(first, second):
        return jnp.where((row == first) | (row == second), 1.0, 0.0)

    main = one_hot(places[0][0], places[1][0])
    tails = [
        one_hot(places[0][1] + TAIL_ROWS * q, places[1][1] + TAIL_ROWS * q) for q in range(4)
    ]
    main = main.astype(BF16)
    copies = []

    def send(k, low, size):
        part = pl.ds(low, size)
        copies.append(pltpu.make_async_copy(out_ref.at[:, part], out_hbm.at[:, part], sems.at[k]))
        copies[-1].start()

    for g in range(4):
        value = dot(main, normed[:, 2 * LANES * g : 2 * LANES * (g + 1)]).astype(BF16)
        for b in range(2):
            low = HEAD_ROWS * (2 * g + b)
            out_ref[:, low : low + HEAD_ROWS, :] = value[:, LANES * b : LANES * (b + 1)].reshape(
                N_EXP, HEAD_ROWS, LANES
            )
        send(g, 2 * HEAD_ROWS * g, 2 * HEAD_ROWS)
    tail = jnp.zeros((N_EXP * HEAD_ROWS, 2 * LANES), F32)
    for q in range(4):
        pair = jnp.concatenate(
            [
                normed[:, LANES * q : LANES * (q + 1)],
                normed[:, LANES * (q + 4) : LANES * (q + 5)],
            ],
            axis=1,
        )
        tail = tail + dot(tails[q].astype(BF16), pair)
    store_tail(out_ref, tail.astype(BF16))
    send(4, N_BLK * HEAD_ROWS, 2 * HEAD_ROWS)
    for copy in copies:
        copy.wait()


def tail_pick(q):
    shape = (N_EXP * TAIL_ROWS, N_EXP * HEAD_ROWS)
    r, col = (iota(shape, 0), iota(shape, 1))
    source = (r // TAIL_ROWS) * HEAD_ROWS + TAIL_ROWS * q + r % TAIL_ROWS
    return (source == col).astype(BF16)


def unpacked(ref):
    tails = load_tail(ref)
    picked = [dot(tail_pick(q), tails).astype(BF16) for q in range(4)]
    tail = jnp.concatenate(
        [p[:, LANES * g : LANES * (g + 1)] for g in range(2) for p in picked], axis=1
    )
    return jnp.concatenate([load_main(ref), tail], axis=0)


def first_half_kernel(core_ref, up_hbm, own_ref, gate_ref, gate_out, up_out, up_ref, sem):
    half = gate_ref.shape[1] // 2
    low = pl.multiple_of(core_ref[0] * half, half)
    copy = pltpu.make_async_copy(up_hbm.at[:, pl.ds(low, half)], up_ref, sem)
    copy.start()
    rows = unpacked(own_ref)
    gate_out[...] = over_last(rows, gate_ref[:, pl.ds(low, half)])
    copy.wait()
    up_out[...] = over_last(rows, up_ref[...])


def down_columns(down_ref, parity):
    parts = []
    for j in range(N_BLK):
        low = pl.multiple_of((2 * j + parity) * LANES, LANES)
        parts.append(down_ref[:, pl.ds(low, LANES)])
    return jnp.concatenate(parts, axis=1)


def second_half_kernel(
    core_ref, other_ref, gate_ref, up_ref, gate_in, up_in, hidden_out
):
    half = gate_ref.shape[1] // 2
    other = 1 - core_ref[0]
    low = pl.multiple_of(other * half, half)
    rows = unpacked(other_ref)
    gate = gate_in[...] + over_last(rows, gate_ref[:, pl.ds(low, half)])
    up = up_in[...] + over_last(rows, up_ref[:, pl.ds(low, half)])
    hidden = (gate * jax.nn.sigmoid(gate) * up).astype(BF16)
    hidden_out[...] = hidden


def pick_kernel(core_ref, down_ref, own_out, other_out):
    own_out[...] = down_columns(down_ref, core_ref[0])
    other_out[...] = down_columns(down_ref, 1 - core_ref[0])


def own_down_kernel(hidden_ref, down_ref, out_ref):
    out_ref[...] = dot(hidden_ref[...], down_ref[...])


def other_down_kernel(hidden_ref, down_ref, own_ref, out_hbm, out_ref, sems):
    copies = []
    for g in range(4):
        columns = slice(2 * LANES * g, 2 * LANES * (g + 1))
        value = own_ref[:, columns] + dot(hidden_ref[...], down_ref[:, columns])
        out_ref[2 * g] = value[:, :LANES].astype(BF16)
        out_ref[2 * g + 1] = value[:, LANES:].astype(BF16)
        pair = pl.ds(2 * g, 2)
        copies.append(pltpu.make_async_copy(out_ref.at[pair], out_hbm.at[pair], sems.at[g]))
        copies[-1].start()
    for copy in copies:
        copy.wait()


def collect_kernel(parts_ref, out_ref):
    total = parts_ref[0].astype(F32)
    for j in range(1, N_BLK):
        total = total + parts_ref[j].astype(F32)
    total = total.astype(BF16)
    rows = N_EXP * HEAD_ROWS
    out_ref[:, :HEAD_ROWS, :] = total[:rows].reshape(N_EXP, HEAD_ROWS, LANES)
    shape = (N_EXP * 8, N_EXP * TAIL_ROWS)
    r, col = (iota(shape, 0), iota(shape, 1))
    spread = (r // 8 * TAIL_ROWS + r % 8 == col) & (r % 8 < TAIL_ROWS)
    tail = dot(spread.astype(BF16), total[rows:]).reshape(N_EXP, 8, LANES)
    out_ref[:, HEAD_ROWS:, :] = tail.astype(BF16)


def weights_kernel(routes_ref, logit_ref, out_ref):
    tokens = routes_ref.shape[0]
    routes = routes_ref[...]
    logit = logit_ref[...]
    expert = iota((tokens, N_EXP), 1)
    picks = [(routes[:, k : k + 1] == expert).astype(F32) for k in range(2)]
    before = (iota((tokens, tokens), 1) < iota((tokens, tokens), 0)).astype(BF16)
    ranks = dot(before, (picks[0] + picks[1]).astype(BF16))
    rows = N_EXP * HEAD_ROWS
    col = iota((tokens, rows + N_EXP * 8), 1)
    total = jnp.zeros(col.shape, F32)
    for k in range(2):
        weight = jax.nn.sigmoid(logit[:, k : k + 1] - logit[:, 1 - k : 2 - k])
        rank = jnp.sum(ranks * picks[k], axis=1, keepdims=True).astype(jnp.int32)
        route = routes[:, k : k + 1]
        place = jnp.where(
            rank < HEAD_ROWS,
            route * HEAD_ROWS + rank,
            rows + route * 8 + rank - HEAD_ROWS,
        )
        total = total + jnp.where(col == place, weight, 0.0)
    high = total.astype(BF16)
    out_ref[0] = high
    out_ref[1] = (total - high.astype(F32)).astype(BF16)


def combine_kernel(back_ref, weight_ref, out_ref):
    rows = N_EXP * HEAD_ROWS
    back = jnp.concatenate(
        [
            back_ref[:, :HEAD_ROWS, :].reshape(rows, LANES),
            back_ref[:, HEAD_ROWS:, :].reshape(N_EXP * 8, LANES),
        ],
        axis=0,
    )
    out_ref[...] = (dot(weight_ref[0], back) + dot(weight_ref[1], back)).astype(BF16)


def exchange(value, axes):
    return lax.all_to_all(value, axes, split_axis=0, concat_axis=0, tiled=True)


def from_behind(value, steps):
    count = lax.axis_size(EP)
    return lax.ppermute(value, EP, [(k, k + steps) for k in range(count - steps)])


def rows_behind(value, steps):
    count = lax.axis_size("z")
    return lax.ppermute(value, "z", [(k, k + steps) for k in range(count - steps)])


def join(after, before):
    return call(join_kernel, sds(after.shape, BF16), (after, before), 10**8, vmem=4)


def swap_cores(value):
    return lax.ppermute(value, "c", [(0, 1), (1, 0)])


def in_hbm(*arrays):
    return tuple(pltpu.with_memory_space_constraint(a, pltpu.HBM) for a in arrays)


def first_loads(group, x_in, b_in, c_in, moe_rows, moe_gain, routes):
    rows = x_in.shape[0] + 2 * NSTATE
    given = in_hbm(x_in, b_in, c_in, moe_rows, moe_gain[None, :], routes.T)
    return call(
        rim_kernel,
        (sds((8, rows), BF16), *(sds(a.shape, a.dtype) for a in given[3:])),
        (group, *given),
        10**8,
        smem=1,
        hbm=6,
        vmem=4,
        scratch=(
            pltpu.VMEM((x_in.shape[0], LANES), BF16),
            pltpu.VMEM((NSTATE, LANES), BF16),
            pltpu.VMEM((NSTATE, LANES), BF16),
            pltpu.SemaphoreType.DMA((6,)),
        ),
    )


def down_halves(core, down):
    half = sds((down.shape[0], down.shape[1] // 2), BF16)
    own, theirs = call(pick_kernel, (half, half), (core, down), 10**8, smem=1)
    return own, swap_cores(theirs)


def run_experts(core, own, w_gate, w_up, down_own, down_other):
    rows, hidden_units = (N_EXP * CAP, w_gate.shape[2])
    gate, up = (w_gate[0].T, w_up[0].T)
    other = swap_cores(own)
    half_act = sds((rows, hidden_units), F32)
    gate_act, up_act = call(
        first_half_kernel,
        (half_act, half_act),
        (core, *in_hbm(up), own, gate),
        10**9,
        smem=1,
        hbm=1,
        vmem=20,
        scratch=(pltpu.VMEM((up.shape[0], up.shape[1] // 2), BF16), pltpu.SemaphoreType.DMA),
    )
    hidden = call(
        second_half_kernel,
        sds((rows, hidden_units), BF16),
        (core, other, gate, up, gate_act, up_act),
        2 * 10**9,
        smem=1,
        vmem=20,
    )
    partner = swap_cores(hidden)
    mine = call(
        own_down_kernel,
        sds((rows, down_own.shape[1]), F32),
        (hidden, down_own),
        6 * 10**8,
        vmem=12,
    )
    return call(
        other_down_kernel,
        sds((N_BLK, rows, LANES), BF16),
        (partner, down_other, mine),
        6 * 10**8,
        out_hbm=True,
        vmem=12,
        scratch=(pltpu.VMEM((N_BLK, rows, LANES), BF16), pltpu.SemaphoreType.DMA((4,))),
    )


def rim_kernel(
    group_ref, x_hbm, b_hbm, c_hbm, rows_hbm, gain_hbm, routes_hbm,
    out_ref, rows_out, gain_out, routes_out, x_ref, b_ref, c_ref, sems,
):
    group = pl.ds(pl.multiple_of(group_ref[0] * NSTATE, NSTATE), NSTATE)
    last = pl.ds(x_hbm.shape[1] - LANES, LANES)
    pairs = (
        (x_hbm.at[:, last], x_ref),
        (b_hbm.at[group, last], b_ref),
        (c_hbm.at[group, last], c_ref),
        (rows_hbm, rows_out),
        (gain_hbm, gain_out),
        (routes_hbm, routes_out),
    )
    copies = [
        pltpu.make_async_copy(source, target, sems.at[k]) for k, (source, target) in enumerate(pairs)
    ]
    for copy in copies:
        copy.start()
    for copy in copies[:3]:
        copy.wait()
    rows = jnp.concatenate([r[...].astype(F32) for r in (x_ref, b_ref, c_ref)], axis=0)
    out_ref[...] = rows.T[LANES - 8 :, :].astype(BF16)
    for copy in copies[3:]:
        copy.wait()


def conv(signal, rim, taps):
    length = signal.shape[1]
    joined = jnp.concatenate([rim, signal], axis=1)
    total = taps[:, TAPS - 1 : TAPS] * signal
    for back in range(1, TAPS):
        moved = pltpu.roll(joined, back, axis=1)[:, LANES : LANES + length]
        total = total + taps[:, TAPS - 1 - back : TAPS - back] * moved
    return total * jax.nn.sigmoid(total)


def upright(taps):
    return jnp.concatenate([taps, jnp.zeros((4, taps.shape[1]), F32)], axis=0).T


def over_first(a, b):
    return lax.dot_general(a, b, (((0,), (0,)), ((), ())), preferred_element_type=F32)


def over_last(a, b):
    return lax.dot_general(a, b, (((1,), (1,)), ((), ())), preferred_element_type=F32)


def local_kernel(
    group_ref, x_hbm, b_hbm, c_hbm, rim_ref, dt_ref, rate_ref, tx_ref, tb_ref, tc_ref,
    x_out, b_out, c_out, cum_out, step_out, sent_out, x_ref, b_ref, c_ref, sems,
):
    heads, length = dt_ref.shape
    values = x_ref.shape[0]
    low = pl.multiple_of(group_ref[0] * NSTATE, NSTATE)
    own = pl.ds(low, NSTATE)
    fetch(((x_hbm, x_ref), (b_hbm.at[own], b_ref), (c_hbm.at[own], c_ref)), sems)
    rim = jnp.concatenate(
        [jnp.zeros((LANES - 8, values + 2 * NSTATE), F32), rim_ref[...].astype(F32)], axis=0
    ).T
    x = conv(x_ref[...].astype(F32), rim[:values], upright(tx_ref[...]))
    b_rim = rim[values : values + NSTATE]
    b = conv(b_ref[...].astype(F32), b_rim, upright(tb_ref[:, own])).astype(BF16)
    c_rim = rim[values + NSTATE :]
    c = conv(c_ref[...].astype(F32), c_rim, upright(tc_ref[:, own])).astype(BF16)
    raw = dt_ref[...]
    step = jnp.maximum(raw, 0.0) + jnp.log1p(jnp.exp(-jnp.abs(raw)))
    cum = -step * rate_ref[...]
    lane = iota((heads, length), 1)
    move = 1
    while move < length:
        cum = cum + jnp.where(lane >= move, pltpu.roll(cum, move, axis=1), 0.0)
        move *= 2
    x16 = x.astype(BF16)
    x_out[...] = x16
    b_out[...] = b
    c_out[...] = c
    cum_out[...] = cum
    step_out[...] = step
    end = cum[:, length - 1 : length]
    tail = jnp.exp(end - cum) * step
    sends = []
    for h in range(heads):
        rows = slice(HEAD_DIM * h, HEAD_DIM * (h + 1))
        weighted = (x[rows] * tail[h : h + 1]).astype(BF16)
        state = over_last(weighted, b)
        total = jnp.exp(end[h : h + 1])
        high = total.astype(BF16).astype(F32)
        sent_out[rows, :] = state.astype(BF16)
        sends += [high, total - high]
    sent_out[heads * HEAD_DIM :, :] = in_rows(sends).astype(BF16)


def in_rows(values):
    row = iota((16, LANES), 0)
    total = jnp.zeros((16, LANES), F32)
    for k, value in enumerate(values):
        total = jnp.where(row == k, value, total)
    return total


def inner_kernel(x_ref, b_ref, c_ref, cum_ref, step_ref, y_out):
    heads, length = cum_ref.shape
    cum = cum_ref[...]
    pad = jnp.zeros((LANES - 2 * heads, length), F32)
    columns = jnp.concatenate([cum, step_ref[...], pad], axis=0).T
    score = over_first(b_ref[...], c_ref[...])
    for h in range(heads):
        rows = slice(HEAD_DIM * h, HEAD_DIM * (h + 1))
        for t in range(length // LANES):
            here = slice(LANES * t, LANES * (t + 1))
            size = LANES * (t + 1)
            gap = cum[h : h + 1, here] - columns[:size, h : h + 1]
            inside = iota((size, LANES), 0) <= iota((size, LANES), 1) + LANES * t
            decay = jnp.exp(jnp.where(inside, gap, -1e30))
            mask = score[:size, here] * decay * columns[:size, heads + h : heads + h + 1]
            y_out[rows, here] = dot(x_ref[rows, :size], mask.astype(BF16))


def state_and_decays(ref):
    size = ref.shape[0] - 16
    value = ref[...].astype(F32)
    pairs = range(size, size + 2 * (size // HEAD_DIM), 2)
    return value[:size], [value[k : k + 1] + value[k + 1 : k + 2] for k in pairs]


def joined(after, before):
    states = [
        after[0][HEAD_DIM * h : HEAD_DIM * (h + 1)] + d * before[0][HEAD_DIM * h : HEAD_DIM * (h + 1)]
        for h, d in enumerate(after[1])
    ]
    return jnp.concatenate(states, axis=0), [a * b for a, b in zip(after[1], before[1])]


def store_spans(ref, value):
    size = ref.shape[0] - 16
    ref[:size, :] = value[0].astype(BF16)
    rows = []
    for total in value[1]:
        high = total.astype(BF16).astype(F32)
        rows += [high, total - high]
    ref[size:, :] = in_rows(rows).astype(BF16)


def join_kernel(after_ref, before_ref, out_ref):
    store_spans(out_ref, joined(state_and_decays(after_ref), state_and_decays(before_ref)))


def row_kernel(place_ref, own_ref, first_ref, second_ref, third_ref, before_out, total_out):
    place = place_ref[0]
    sources = [state_and_decays(r) for r in (own_ref, first_ref, second_ref, third_ref)]
    heads = len(sources[0][1])
    running = (jnp.zeros(sources[0][0].shape, F32), [jnp.ones((1, LANES), F32)] * heads)
    before = running
    for j in range(4):
        back = (place - j) & 3
        state, decays = sources[0]
        for k in range(1, 4):
            here = back == k
            state = jnp.where(here, sources[k][0], state)
            decays = [jnp.where(here, a, b) for a, b in zip(sources[k][1], decays)]
        running = joined((state, decays), running)
        ahead = j < place
        before = (
            jnp.where(ahead, running[0], before[0]),
            [jnp.where(ahead, a, b) for a, b in zip(running[1], before[1])],
        )
    store_spans(before_out, before)
    store_spans(total_out, running)


def mixed_kernel(y_ref, row_ref, far_ref, c_ref, cum_ref, z_ref, gain_ref, out_ref):
    heads = cum_ref.shape[0]
    reach = jnp.exp(cum_ref[...])
    before = joined(state_and_decays(row_ref), state_and_decays(far_ref))[0]
    carried = dot(before.astype(BF16), c_ref[...])
    for h in range(heads):
        rows = slice(HEAD_DIM * h, HEAD_DIM * (h + 1))
        z = z_ref[rows, :].astype(F32)
        y = y_ref[rows, :] + carried[rows] * reach[h : h + 1]
        gated = y * (z * jax.nn.sigmoid(z))
        scale = lax.rsqrt(jnp.mean(gated * gated, axis=0, keepdims=True) + HEAD_EPS)
        out_ref[rows, :] = (gated * scale * gain_ref[rows, :]).astype(BF16)


def on_device(
    x_in,
    z_in,
    dt_raw,
    decay_rate,
    b_in,
    c_in,
    conv_x,
    conv_b,
    conv_c,
    head_gain,
    moe_rows,
    moe_gain,
    routes,
    route_logit,
    w_gate,
    w_up,
    w_down,
):
    heads, length = dt_raw.shape
    values = x_in.shape[0]
    core = lax.axis_index("c").astype(jnp.int32)[None]
    group = lax.axis_index(TP) * heads // (HEADS // GROUPS)
    group = group.astype(jnp.int32)[None]
    own_rim, *tokens = first_loads(group, x_in, b_in, c_in, moe_rows, moe_gain, routes)
    rims = from_behind(own_rim, 1)
    outbox = call(
        prep_kernel,
        sds((N_EXP, CHUNK, LANES), BF16),
        (core, *tokens),
        5 * 10**8,
        smem=1,
        out_hbm=True,
        scratch=(pltpu.VMEM((N_EXP, CHUNK, LANES), BF16), pltpu.SemaphoreType.DMA((5,))),
    )
    arrived = exchange(outbox, EP)
    down_parts = down_halves(core, w_down[0])
    x_conv, b_conv, c_conv, cum, step_dt, sent = call(
        local_kernel,
        (
            sds((values, length), BF16),
            sds((NSTATE, length), BF16),
            sds((NSTATE, length), BF16),
            sds((heads, length), F32),
            sds((heads, length), F32),
            sds((values + 16, LANES), BF16),
        ),
        (
            group, x_in, b_in, c_in, rims, dt_raw, decay_rate[:, None],
            conv_x.T, conv_b.T, conv_c.T,
        ),
        2 * 10**9,
        smem=1,
        hbm=3,
        scratch=(
            pltpu.VMEM((values, length), BF16),
            pltpu.VMEM((NSTATE, length), BF16),
            pltpu.VMEM((NSTATE, length), BF16),
            pltpu.SemaphoreType.DMA((3,)),
        ),
    )
    in_order = [
        lax.ppermute(sent, "x", [(k, (k + step) % 4) for k in range(4)]) for step in (1, 2, 3)
    ]
    y_local = call(
        inner_kernel,
        sds((values, length), F32),
        (x_conv, b_conv, c_conv, cum, step_dt),
        2 * 10**8,
    )
    in_row, spans = call(
        row_kernel,
        (sds(sent.shape, BF16), sds(sent.shape, BF16)),
        (lax.axis_index("x").astype(jnp.int32)[None], sent, *in_order),
        10**8,
        smem=1,
    )
    nearest = rows_behind(spans, 1)
    second = rows_behind(spans, 2)
    spans = join(nearest, second)
    for steps in (2, 4):
        behind = rows_behind(spans, steps)
        spans = join(spans, behind)
    weights = call(
        weights_kernel,
        sds((2, moe_rows.shape[0], N_EXP * (HEAD_ROWS + 8)), BF16),
        (routes, route_logit),
        10**9,
    )
    partial = run_experts(core, arrived, w_gate, w_up, *down_parts)
    parts = exchange(partial, "y")
    collected = call(
        collect_kernel, sds((N_EXP, HEAD_ROWS + 8, LANES), BF16), (parts,), 10**8
    )
    back = exchange(collected, EP)
    mixed = call(
        mixed_kernel,
        sds((values, length), BF16),
        (y_local, in_row, spans, c_conv, cum, z_in, head_gain[:, None]),
        2 * 10**9,
    )
    moe_out = call(
        combine_kernel, sds((moe_rows.shape[0], LANES), BF16), (back, weights), 10**8
    ).T
    return (mixed, moe_out)


def solution(mesh):
    finer = Mesh(mesh.devices.reshape(8, 4, 8, 2), ("z", "x", "y", "c"))
    in_specs = (
        P(TP, EP),
        P(TP, EP),
        P(TP, EP),
        P(TP),
        P(None, EP),
        P(None, EP),
        P(TP, None),
        P(),
        P(),
        P(TP),
        P(EP, None),
        P(),
        P(EP, None),
        P(EP, None),
        P(EP, None, TP),
        P(EP, None, TP),
        P(EP, TP, None),
    )
    out_specs = (P(TP, EP), P(TP, EP))

    return jax.shard_map(
        on_device, mesh=finer, in_specs=in_specs, out_specs=out_specs, check_vma=False
    )
```
